32 devices in a mesh: sp: 8 (over z, y), dp: 4 (over x, core).
Axes of the slice: x: 2, y: 2, z: 4, core: 2. Of those that a mesh axis runs over, the one named last changes fastest.
Arguments:
- queries: bfloat16 [4, 1024, 16, 128], P('dp', 'sp'), may hold values from -7 to 7
- key_vectors: bfloat16 [4, 1024, 16, 128], P('dp', 'sp'), may hold values from -6 to 6
- value_vectors: bfloat16 [4, 1024, 16, 128], P('dp', 'sp'), may hold values from -6 to 6
- head_lambda: float32 [16], P('sp'), may hold values from 0.3 to 0.8
- head_gain: float32 [128], replicated, may hold values from 0.1 to 1.9
- residual: bfloat16 [4, 1024, 2048], P('dp', 'sp'), may hold values from -6 to 6
- out_weight: bfloat16 [2048, 2048], replicated, may hold values from -0.125 to 0.125
- mix_gain: float32 [2048], replicated, may hold values from 0.1 to 1.9
- pre_gain: float32 [2048], replicated, may hold values from 0.1 to 1.9
- post_gain: float32 [2048], replicated, may hold values from 0.1 to 1.9
- routes: int32 [4, 1024, 4], P('dp', 'sp'), may hold values from 0 to 31, all different within a row; in each aligned block of 128 rows (0 to 127, 128 to 255, ..., all dimensions but the last counted through in order) at most 24 rows name the same one
- route_weights: float32 [4, 1024, 4], P('dp', 'sp'), may hold values from 0.25 to 1
- expert_gate: bfloat16 [32, 2048, 512], P(('sp', 'dp')), may hold values from -0.125 to 0.125
- expert_up: bfloat16 [32, 2048, 512], P(('sp', 'dp')), may hold values from -0.125 to 0.125
- expert_down: bfloat16 [32, 512, 2048], P(('sp', 'dp')), may hold values from -0.25 to 0.25
- shared_gate: bfloat16 [2048, 512], replicated, may hold values from -0.125 to 0.125
- shared_up: bfloat16 [2048, 512], replicated, may hold values from -0.125 to 0.125
- shared_down: bfloat16 [512, 2048], replicated, may hold values from -0.25 to 0.25
Outputs:
- output: bfloat16 [4, 1024, 2048], P('dp', 'sp')
The draws below stay inside these ranges and needn't reach their ends.
Inputs may be any that keep to these rules, and one draw needn't show every extreme that they name: `routes`: among the tokens of one device (aligned blocks of 128 positions), no expert is named more than 24 times; in some block some expert is named exactly 24 times. Each token names 4 different experts.
All inputs are finite; a program needn't handle non-finite values.
Results may differ from the reference program's by a relative error of at most 0.0075.
Values may be sent and summed in bfloat16 or wider, within the bound.
A program may use at most 128 MiB of HBM per device.

```python
import math
import jax
import jax.numpy as jnp
import numpy as np
from jax import lax

D = 2048
HEADS = 16
HD = 64
VD = 128
FF = 512
TOP_K = 4
TOK_DEV = 128
LEN = 1024
SEQS = 4
EXPERTS = 32
CAP = 24


def draw_queries(key, part):
    shape = (SEQS, LEN, HEADS, 2 * HD)
    base_key = jax.random.fold_in(key, 11)
    drawn = jnp.clip(1.75 * jax.random.normal(base_key, shape, jnp.float32), -7.0, 7.0)
    return drawn.astype(jnp.bfloat16)


def draw_key_vectors(key, part):
    shape = (SEQS, LEN, HEADS, 2 * HD)
    base_key = jax.random.fold_in(key, 13)
    drawn = jnp.clip(jax.random.normal(base_key, shape, jnp.float32), -6.0, 6.0)
    return drawn.astype(jnp.bfloat16)


def levels(key, dims, cuts, least, top_value):
    def one(position, parts):
        draws = jax.random.uniform(jax.random.fold_in(jax.random.fold_in(key, 6), position), (parts,), jnp.float32, least / len(cuts), top_value / len(cuts))
        return jnp.repeat(jnp.exp(draws), dims[position] // parts).reshape((-1,) + (1,) * (len(dims) - position - 1))

    level = one(*cuts[0])
    for cut in cuts[1:]:
        level = level * one(*cut)
    return level


def deal_out(rng, own, number, rows, amount, top, reach, slope):
    sequence = jax.random.permutation(rng, amount)
    heavy_load, common = portions_of(amount, rows * top, reach, slope, True), portions_of(amount, rows * top, reach, slope, False)
    places = jnp.arange(amount)

    def named(lengths, rotation):
        used = int((lengths > 0).sum())
        fixed = max(1, used // 4)
        passed = fixed + (places - fixed + rotation * (used - fixed)) % max(1, amount - fixed)
        return jnp.zeros((amount,), jnp.int32).at[sequence[jnp.where(places < fixed, places, passed)]].set(jnp.asarray(lengths, jnp.int32))

    lengths = jnp.where(number % 4 == 0, named(heavy_load, number // 4), named(common, number - number // 4 - 1))
    mixed = jax.random.permutation(jax.random.fold_in(own, 3), amount)
    source_of, sink = mixed[0:amount // 2 * 2:2], mixed[1:amount // 2 * 2:2]
    room = jnp.minimum(lengths[source_of] - 1, reach - lengths[sink]) // 2
    room = jnp.where((source_of == sequence[0]) | (sink == sequence[0]) | (lengths[sink] == 0), 0, jnp.maximum(room, 0))
    passed = jax.random.randint(jax.random.fold_in(own, 4), (amount // 2,), 0, 1 << 20) % (room + 1)
    lengths = lengths.at[source_of].add(-passed).at[sink].add(passed)
    members = jnp.searchsorted(jnp.cumsum(lengths), jnp.arange(rows * top), side="right").astype(jnp.int32)
    listing = members.reshape(top, rows).T
    listing = listing[jax.random.permutation(jax.random.fold_in(own, 1), rows)]
    rotation = jax.random.randint(jax.random.fold_in(own, 2), (rows, 1), 0, top)
    return jnp.take_along_axis(listing, (jnp.arange(top)[None, :] + rotation) % top, axis=1)


def portions_of(count, total, reach, lean, full):
    weights = [(1 << 20) // math.isqrt(grade ** lean) + 1 for grade in range(1, count + 1)]
    largest = reach if full else min(reach, max(-(-total // count), total * weights[0] // sum(weights)))
    least = 1 if total - largest >= count - 1 else 0
    counts, spare = [largest] + [least] * (count - 1), total - largest - least * (count - 1)
    while spare > 0:
        candidates = [i for i in range(1, count) if counts[i] < largest] or [i for i in range(1, count) if counts[i] < reach]
        whole, remaining = sum([weights[i] for i in candidates]), spare
        for i in candidates:
            extra = min(reach - counts[i], max(1, remaining * weights[i] // whole), spare)
            counts[i] = counts[i] + extra
            spare = spare - extra
    return np.array(counts)


def bell_draw(rng, dims, spread, reach, pieces=(), held_as=jnp.bfloat16):
    values = spread * jax.random.normal(rng, dims, jnp.float32)
    if pieces:
        values = values * levels(rng, dims, pieces, -0.22, 0.18)
    return jnp.clip(values, -reach, reach).astype(held_as)


def setup_inputs(seed: int = 0) -> dict:
    key_list = jax.random.split(jax.random.key(seed), 19)
    queries = draw_queries(jax.random.fold_in(key_list[18], 71), 0)
    key_vectors = draw_key_vectors(jax.random.fold_in(key_list[18], 71), 0)
    value_vectors = bell_draw(key_list[2], (SEQS, LEN, HEADS, VD), 1.0, 6.0, ((0, 4), (1, 8)))
    head_lambda = jnp.clip(0.3 + 0.5 * jax.random.uniform(key_list[3], (HEADS,), jnp.float32) ** levels(key_list[3], (HEADS,), ((0, 8),), -0.2, 0.2), 0.3, 0.8)
    head_gain = jnp.clip(1.0 + 0.18 * jax.random.normal(key_list[4], (VD,), jnp.float32), 0.1, 1.9)
    residual = bell_draw(key_list[5], (SEQS, LEN, D), 1.0, 6.0, ((0, 4), (1, 8)))
    out_weight = bell_draw(key_list[6], (HEADS * VD, D), (HEADS * VD) ** -0.5, 0.125)
    mix_gain = jnp.clip(1.0 + 0.18 * jax.random.normal(key_list[7], (D,), jnp.float32), 0.1, 1.9)
    pre_gain = jnp.clip(1.0 + 0.18 * jax.random.normal(key_list[8], (D,), jnp.float32), 0.1, 1.9)
    post_gain = jnp.clip(1.0 + 0.18 * jax.random.normal(key_list[9], (D,), jnp.float32), 0.1, 1.9)
    routes_keys = jax.random.split(jax.random.fold_in(key_list[10], 1), SEQS * LEN // TOK_DEV)
    routes_turns = jax.random.permutation(jax.random.fold_in(key_list[10], 3), SEQS * LEN // TOK_DEV)
    routes = jax.vmap(lambda own, number: deal_out(jax.random.fold_in(key_list[10], 2), own, number, TOK_DEV, EXPERTS, TOP_K, CAP, 2))(routes_keys, routes_turns).reshape((SEQS, LEN, TOP_K))
    route_weights = jnp.clip(0.25 + 0.75 * jax.random.uniform(key_list[11], (SEQS, LEN, TOP_K), jnp.float32) ** levels(key_list[11], (SEQS, LEN, TOP_K), ((0, 4), (1, 8)), -0.2, 0.2), 0.25, 1.0)
    expert_gate = bell_draw(key_list[12], (EXPERTS, D, FF), D ** -0.5, 0.125, ((0, 32),))
    expert_up = bell_draw(key_list[13], (EXPERTS, D, FF), D ** -0.5, 0.125, ((0, 32),))
    expert_down = bell_draw(key_list[14], (EXPERTS, FF, D), FF ** -0.5, 0.25, ((0, 32),))
    shared_gate = bell_draw(key_list[15], (D, FF), D ** -0.5, 0.125)
    shared_up = bell_draw(key_list[16], (D, FF), D ** -0.5, 0.125)
    shared_down = bell_draw(key_list[17], (FF, D), FF ** -0.5, 0.25)
    return dict(queries=queries, key_vectors=key_vectors, value_vectors=value_vectors, head_lambda=head_lambda, head_gain=head_gain, residual=residual, out_weight=out_weight, mix_gain=mix_gain, pre_gain=pre_gain, post_gain=post_gain, routes=routes, route_weights=route_weights, expert_gate=expert_gate, expert_up=expert_up, expert_down=expert_down, shared_gate=shared_gate, shared_up=shared_up, shared_down=shared_down)


epsilon = 1e-06

def rms_scale(values_in, gain):
    return values_in * lax.rsqrt(lax.optimization_barrier(jnp.mean(values_in * values_in, axis=-1, keepdims=True)) + epsilon) * gain

def feed_forward(rows, gate_w, up_w, down_w):
    gate_val = jnp.dot(rows, gate_w, preferred_element_type=jnp.float32)
    up_val = jnp.dot(rows, up_w, preferred_element_type=jnp.float32)
    hidden = (jax.nn.silu(gate_val) * up_val).astype(jnp.bfloat16)
    return jnp.dot(hidden, down_w, preferred_element_type=jnp.float32).astype(jnp.bfloat16)

def attend_sequence(query_seq, key_seq, value_seq, head_lambda, head_gain):
    length = query_seq.shape[0]
    head_count = query_seq.shape[1]
    head_size = query_seq.shape[2] // 2
    block_rows = min(512, length)
    block_count = length // block_rows
    query_blocks = query_seq.astype(jnp.float32).reshape(block_count, block_rows, head_count, 2, head_size)
    key_all = key_seq.astype(jnp.float32).reshape(length, head_count, 2, head_size)
    value_all = value_seq.astype(jnp.float32)
    key_pos = jnp.arange(length, dtype=jnp.int32)

    def one_block(inputs):
        query_block, block_index = inputs
        scores = jnp.einsum('qhmd,khmd->hmqk', query_block, key_all) * head_size ** (-0.5)
        query_pos = block_index * block_rows + jnp.arange(block_rows, dtype=jnp.int32)
        causal = key_pos[None, :] <= query_pos[:, None]
        scores = jnp.where(causal, scores, -jnp.inf)
        maxima = lax.optimization_barrier(jnp.max(scores, axis=-1, keepdims=True))
        exponent = jnp.exp(scores - maxima)
        softmax_both = exponent / lax.optimization_barrier(jnp.sum(exponent, axis=-1, keepdims=True))
        mixture = softmax_both[:, 0] - head_lambda[:, None, None] * softmax_both[:, 1]
        mixture_low = lax.optimization_barrier(mixture.astype(jnp.bfloat16)).astype(jnp.float32)
        head_output = jnp.einsum('hqk,khe->qhe', mixture_low, value_all)
        return rms_scale(head_output, head_gain).astype(jnp.bfloat16)
    outputs = lax.map(one_block, (query_blocks, jnp.arange(block_count, dtype=jnp.int32)))
    return outputs.reshape(length, head_count, -1)

def reference(queries, key_vectors, value_vectors, head_lambda, head_gain, residual, out_weight, mix_gain, pre_gain, post_gain, routes, route_weights, expert_gate, expert_up, expert_down, shared_gate, shared_up, shared_down):
    heads_out = lax.map(lambda inputs: attend_sequence(inputs[0], inputs[1], inputs[2], head_lambda, head_gain), (queries, key_vectors, value_vectors))
    token_total = SEQS * LEN
    flat_heads = heads_out.reshape(token_total, HEADS * VD)
    mixed_rows = jnp.dot(flat_heads, out_weight, preferred_element_type=jnp.float32)
    updated = (residual.reshape(token_total, D).astype(jnp.float32) + rms_scale(mixed_rows, mix_gain)).astype(jnp.bfloat16)
    normed = rms_scale(updated.astype(jnp.float32), pre_gain).astype(jnp.bfloat16)
    shared_out = feed_forward(normed, shared_gate, shared_up, shared_down)
    block_total = token_total // TOK_DEV
    assign_block = TOK_DEV * TOP_K
    flat_routes = routes.reshape(block_total, assign_block).astype(jnp.int32)
    one_hot = (flat_routes[:, :, None] == jnp.arange(EXPERTS, dtype=jnp.int32)[None, None, :]).astype(jnp.int32)
    earlier = jnp.cumsum(one_hot, axis=1) - one_hot
    rank_index = lax.optimization_barrier(jnp.sum(earlier * one_hot, axis=2))
    block_ids = jnp.arange(block_total, dtype=jnp.int32)[:, None]
    slot_index = (flat_routes * (block_total * CAP) + block_ids * CAP + rank_index).reshape(-1)
    assign_ids = jnp.arange(block_total * assign_block, dtype=jnp.int32)
    source_table = jnp.zeros((EXPERTS * block_total * CAP,), jnp.int32).at[slot_index].set(assign_ids)
    rows_per_expert = source_table.reshape(EXPERTS, block_total * CAP) // TOP_K

    def run_expert(inputs):
        row_ids, gate_w, up_w, down_w = inputs
        return feed_forward(normed[row_ids], gate_w, up_w, down_w)
    expert_out = lax.map(run_expert, (rows_per_expert, expert_gate, expert_up, expert_down))
    picked = expert_out.reshape(EXPERTS * block_total * CAP, D)[slot_index]
    routed = lax.optimization_barrier(jnp.sum(picked.astype(jnp.float32).reshape(token_total, TOP_K, D) * route_weights.reshape(token_total, TOP_K, 1), axis=1))
    combined = routed + shared_out.astype(jnp.float32)
    output = (updated.astype(jnp.float32) + rms_scale(combined, post_gain)).astype(jnp.bfloat16)
    return output.reshape(SEQS, LEN, D)
```

```python
import functools

import jax
import jax.numpy as jnp
from jax import lax
from jax.experimental import pallas as pl
from jax.experimental.pallas import tpu as pltpu
from jax.sharding import PartitionSpec as P

epsilon = 1e-06
MESH = pl.DeviceIdType.MESH
VMEM = pl.BlockSpec(memory_space=pltpu.VMEM)


def rms_scale(values_in, gain):
    return (
        values_in
        * lax.rsqrt(jnp.mean(values_in * values_in, axis=-1, keepdims=True) + epsilon)
        * gain
    )


def columns_of(index, width):
    return pl.ds(pl.multiple_of(index * width, width), width)


def line_barrier(n, me):
    barrier = pltpu.get_barrier_semaphore()

    def greet(off, carry):
        pl.semaphore_signal(
            barrier, inc=1, device_id={"sp": lax.rem(me + off, n)}, device_id_type=MESH
        )
        return carry

    lax.fori_loop(1, n, greet, 0)
    pl.semaphore_wait(barrier, n - 1)


def to_heads_kernel(
    n,
    q_ref,
    k_ref,
    v_ref,
    qo_ref,
    ko_ref,
    vo_ref,
    send_sem,
    recv_sem,
    own_sem,
):
    me = lax.axis_index("sp")
    width = qo_ref.shape[2]
    pairs = ((q_ref, qo_ref), (k_ref, ko_ref), (v_ref, vo_ref))
    line_barrier(n, me)

    def copy(which, off):
        source, target = pairs[which]
        dst = lax.rem(me + off, n)
        return pltpu.make_async_remote_copy(
            src_ref=source.at[:, columns_of(dst, width)],
            dst_ref=target.at[me],
            send_sem=send_sem.at[which, off],
            recv_sem=recv_sem.at[which, off],
            device_id={"sp": dst},
            device_id_type=MESH,
        )

    def own(which):
        source, target = pairs[which]
        return pltpu.make_async_copy(
            source.at[:, columns_of(me, width)], target.at[me], own_sem.at[which]
        )

    def start(off, carry):
        for which in range(3):
            copy(which, off).start()
        return carry

    def finish(off, carry):
        for which in range(3):
            copy(which, off).wait()
        return carry

    lax.fori_loop(1, n, start, 0)
    for which in range(3):
        own(which).start()
    for which in range(3):
        own(which).wait()
    lax.fori_loop(1, n, finish, 0)


def to_heads(n, q, k, v):
    tok, model = q.shape
    width = model // n
    out = jax.ShapeDtypeStruct((n, tok, width), q.dtype)
    return pl.pallas_call(
        functools.partial(to_heads_kernel, n),
        out_shape=[out] * 3,
        in_specs=[VMEM] * 3,
        out_specs=[VMEM] * 3,
        scratch_shapes=[
            pltpu.SemaphoreType.DMA((3, n)),
            pltpu.SemaphoreType.DMA((3, n)),
            pltpu.SemaphoreType.DMA((3,)),
        ],
        compiler_params=pltpu.CompilerParams(
            collective_id=0, has_side_effects=True, vmem_limit_bytes=32 * 2**20
        ),
    )(q, k, v)


def to_tokens_kernel(n, a_ref, o_ref, send_sem, recv_sem, own_sem):
    me = lax.axis_index("sp")
    width = a_ref.shape[2]
    line_barrier(n, me)

    def copy(off):
        dst = lax.rem(me + off, n)
        return pltpu.make_async_remote_copy(
            src_ref=a_ref.at[dst],
            dst_ref=o_ref.at[:, columns_of(me, width)],
            send_sem=send_sem.at[off],
            recv_sem=recv_sem.at[off],
            device_id={"sp": dst},
            device_id_type=MESH,
        )

    def start(off, carry):
        copy(off).start()
        return carry

    def finish(off, carry):
        copy(off).wait()
        return carry

    lax.fori_loop(1, n, start, 0)
    own = pltpu.make_async_copy(a_ref.at[me], o_ref.at[:, columns_of(me, width)], own_sem)
    own.start()
    own.wait()
    lax.fori_loop(1, n, finish, 0)


def to_tokens(n, attended):
    _, tok, width = attended.shape
    return pl.pallas_call(
        functools.partial(to_tokens_kernel, n),
        out_shape=jax.ShapeDtypeStruct((tok, n * width), attended.dtype),
        in_specs=[VMEM],
        out_specs=VMEM,
        scratch_shapes=[
            pltpu.SemaphoreType.DMA((n,)),
            pltpu.SemaphoreType.DMA((n,)),
            pltpu.SemaphoreType.DMA,
        ],
        compiler_params=pltpu.CompilerParams(
            collective_id=1, has_side_effects=True, vmem_limit_bytes=32 * 2**20
        ),
    )(attended)


def attend_kernel(block, q_ref, k_ref, v_ref, lam_ref, gain_ref, o_ref):
    length, width = q_ref.shape
    value_size = gain_ref.shape[1]
    heads = width // value_size
    half = value_size // 2
    lane = lax.broadcasted_iota(jnp.int32, (block, value_size), 1)
    row = lax.broadcasted_iota(jnp.int32, (block, block), 0)
    col = lax.broadcasted_iota(jnp.int32, (block, block), 1)
    causal = col <= row
    contract = (((1,), (1,)), ((), ()))
    for head in range(heads):
        cols = slice(head * value_size, (head + 1) * value_size)
        for step in range(length // block):
            rows = slice(step * block, (step + 1) * block)
            past = step * block
            query = q_ref[rows, cols]
            near, far = [], []
            for which in range(2):
                keep = (lane < half) if which == 0 else (lane >= half)
                part = jnp.where(keep, query, jnp.zeros_like(query))
                s_near = lax.dot_general(
                    part, k_ref[rows, cols], contract, preferred_element_type=jnp.float32
                ) * (half**-0.5)
                s_near = jnp.where(causal, s_near, -jnp.inf)
                top = jnp.max(s_near, axis=-1, keepdims=True)
                if past:
                    s_far = lax.dot_general(
                        part, k_ref[:past, cols], contract, preferred_element_type=jnp.float32
                    ) * (half**-0.5)
                    top = jnp.maximum(top, jnp.max(s_far, axis=-1, keepdims=True))
                e_near = jnp.exp(s_near - top)
                total = jnp.sum(e_near, axis=-1, keepdims=True)
                if past:
                    e_far = jnp.exp(s_far - top)
                    total = total + jnp.sum(e_far, axis=-1, keepdims=True)
                scale = 1.0 / total
                if which == 1:
                    scale = scale * lam_ref[head]
                near.append(e_near * scale)
                if past:
                    far.append(e_far * scale)
            mixture = (near[0] - near[1]).astype(jnp.bfloat16)
            result = jnp.dot(mixture, v_ref[rows, cols], preferred_element_type=jnp.float32)
            if past:
                mixture = (far[0] - far[1]).astype(jnp.bfloat16)
                result += jnp.dot(
                    mixture, v_ref[:past, cols], preferred_element_type=jnp.float32
                )
            o_ref[rows, cols] = rms_scale(result, gain_ref[...]).astype(o_ref.dtype)


def attend(q, k, v, head_lambda, head_gain):
    return pl.pallas_call(
        functools.partial(attend_kernel, min(256, q.shape[0])),
        out_shape=jax.ShapeDtypeStruct(q.shape, q.dtype),
        in_specs=[VMEM] * 3 + [pl.BlockSpec(memory_space=pltpu.SMEM), VMEM],
        out_specs=VMEM,
        compiler_params=pltpu.CompilerParams(vmem_limit_bytes=48 * 2**20),
    )(q, k, v, head_lambda, head_gain.reshape(1, -1))


def drain(ref, sem):
    pltpu.make_async_copy(ref, ref, sem).wait()


def experts_kernel(
    planes,
    inner,
    dp_size,
    chunks,
    top,
    normed_ref,
    updated_ref,
    side_ref,
    gain_ref,
    gate_hbm,
    up_hbm,
    down_hbm,
    sgate_hbm,
    sup_hbm,
    sdown_hbm,
    o_ref,
    gate_w,
    up_w,
    down_w,
    sgate_w,
    sup_w,
    sdown_w,
    sides,
    tokens,
    slots_a,
    slots_b,
    pick,
    high,
    low,
    rows,
    inbox,
    flat,
    hidden,
    outs,
    landed,
    partial,
    sums,
    total,
    load_sem,
    side_send,
    side_recv,
    z_send,
    z_recv,
    out_send,
    out_recv,
    back_send,
    back_recv,
    sum_send,
    sum_recv,
):
    group = inner * dp_size
    _, _, _, cap, width = rows.shape
    tok = normed_ref.shape[0]
    cores = 2 if dp_size % 2 == 0 else 1
    chips = dp_size // cores
    sp, dp = lax.axis_index("sp"), lax.axis_index("dp")
    z, y = sp // inner, lax.rem(sp, inner)
    place = y * dp_size + dp
    last = planes - 1
    has_up, has_down = z < last, z > 0
    is_end = lax.rem(z, last) == 0

    def peer(k):
        core = lax.rem(lax.rem(dp, cores) + lax.rem(k, cores), cores)
        chip = lax.rem(dp // cores + lax.rem(k // cores, chips), chips)
        row = lax.rem(y + k // dp_size, inner)
        there = chip * cores + core
        return row * dp_size + there, {"sp": z * inner + row, "dp": there}

    def column(plane):
        return {"sp": plane * inner + y, "dp": dp}

    def over(first, stop, action):
        lax.fori_loop(first, stop, lambda i, carry: (action(i), carry)[1], 0)

    barrier = pltpu.get_barrier_semaphore()
    over(
        1,
        group,
        lambda k: pl.semaphore_signal(
            barrier, inc=1, device_id=peer(k)[1], device_id_type=MESH
        ),
    )
    for d in range(1, planes):
        pl.semaphore_signal(
            barrier, inc=1, device_id=column(lax.rem(z + d, planes)), device_id_type=MESH
        )
    pl.semaphore_wait(barrier, group - 1 + planes - 1)

    loads = [
        pltpu.make_async_copy(source, target, load_sem.at[index])
        for index, (source, target) in enumerate(
            (
                (sgate_hbm, sgate_w),
                (sup_hbm, sup_w),
                (sdown_hbm, sdown_w),
                (gate_hbm, gate_w),
                (up_hbm, up_w),
                (down_hbm, down_w),
            )
        )
    ]

    def side(d):
        return pltpu.make_async_remote_copy(
            src_ref=side_ref,
            dst_ref=sides.at[z],
            send_sem=side_send.at[d],
            recv_sem=side_recv.at[z],
            device_id=column(lax.rem(z + d, planes)),
            device_id_type=MESH,
        )

    def push(block, chunk, up):
        return pltpu.make_async_remote_copy(
            src_ref=tokens.at[block, chunk],
            dst_ref=tokens.at[block, chunk],
            send_sem=z_send.at[up, block, chunk],
            recv_sem=z_recv.at[block, chunk],
            device_id=column(z + 2 * up - 1),
            device_id_type=MESH,
        )

    def pushes(block, own, action):
        @pl.when(jnp.logical_and(has_up, True if own else block < z))
        def _():
            action(1)

        @pl.when(jnp.logical_and(has_down, True if own else block > z))
        def _():
            action(0)

    def block_of(slot):
        if slot == 0:
            return z
        if slot == 1:
            return 1 + lax.rem(z, 2)
        if slot == 2:
            return lax.rem(2 + 3 * z, 5)
        return 3 * (1 - z // 2)

    def deal(slot, chunk):
        def one(k):
            there, device = peer(k)
            pltpu.make_async_remote_copy(
                src_ref=rows.at[slot, chunk, there],
                dst_ref=inbox.at[slot, chunk, place],
                send_sem=out_send.at[slot, chunk],
                recv_sem=out_recv.at[slot, chunk],
                device_id=device,
                device_id_type=MESH,
            ).start()

        over(1, group, one)

    def give_back(slot, chunk):
        def one(k):
            there, device = peer(k)
            pltpu.make_async_remote_copy(
                src_ref=outs.at[slot, chunk, there],
                dst_ref=landed.at[slot, chunk, place],
                send_sem=back_send.at[slot, chunk],
                recv_sem=back_recv.at[slot, chunk],
                device_id=device,
                device_id_type=MESH,
            ).start()

        over(1, group, one)

    def others(ref, slot, chunk):
        return ref.at[slot, chunk, pl.ds(0, group - 1)]

    def tables(slot, source):
        ids = (z * group).astype(jnp.float32) + lax.broadcasted_iota(
            jnp.int32, (group, tok), 0
        ).astype(jnp.float32)
        member = jnp.zeros((group, tok), jnp.float32)
        weight = jnp.zeros((group, tok), jnp.float32)
        for j in range(top):
            named = source[j : j + 1, :] == ids
            member += jnp.where(named, 1.0, 0.0)
            weight += jnp.where(named, source[top + j : top + j + 1, :], 0.0)
        before = lax.broadcasted_iota(jnp.int32, (tok, tok), 0) < lax.broadcasted_iota(
            jnp.int32, (tok, tok), 1
        )
        earlier = jnp.dot(
            member.astype(jnp.bfloat16),
            jnp.where(before, 1.0, 0.0).astype(jnp.bfloat16),
            preferred_element_type=jnp.float32,
        )
        rank = jnp.where(member > 0, earlier, -1.0)
        seat = lax.broadcasted_iota(jnp.int32, (cap, tok), 0).astype(jnp.float32)
        for e in range(group):
            hit = rank[e : e + 1, :] == seat
            slots_a[e * cap : (e + 1) * cap, :] = jnp.where(hit, 1.0, 0.0)
            slots_b[e * cap : (e + 1) * cap, :] = jnp.where(hit, weight[e : e + 1, :], 0.0)
        pick[slot] = slots_a[...].astype(pick.dtype)
        spread = slots_b[...]
        upper = spread.astype(high.dtype)
        high[slot] = upper
        low[slot] = (spread - upper.astype(jnp.float32)).astype(low.dtype)

    def pick_rows(slot, block, chunk):
        value = jnp.dot(pick[slot], tokens[block, chunk], preferred_element_type=jnp.float32)
        rows[slot, chunk] = value.reshape(group, cap, width).astype(rows.dtype)
        inbox[slot, chunk, place] = rows[slot, chunk, place]
        deal(slot, chunk)

    def collect(slot):
        block = block_of(slot)

        def one(chunk):
            drain(tokens.at[block, chunk], z_recv.at[block, chunk])
            pushes(block, False, lambda up: push(block, chunk, up).start())
            pick_rows(slot, block, chunk)

        over(0, chunks, one)

    tile = min(256, gate_w.shape[1])
    tiles = gate_w.shape[1] // tile

    def hidden_of(source, gates, ups, target):
        def one(index, carry):
            some = columns_of(index, tile)
            gate_val = jnp.dot(source[...], gates[:, some], preferred_element_type=jnp.float32)
            up_val = jnp.dot(source[...], ups[:, some], preferred_element_type=jnp.float32)
            target[:, some] = (jax.nn.silu(gate_val) * up_val).astype(target.dtype)
            return carry

        lax.fori_loop(0, tiles, one, 0)

    def expert(slot, send):
        for chunk in range(chunks):
            drain(others(inbox, slot, chunk), out_recv.at[slot, chunk])
            part = inbox[slot, chunk].astype(jnp.float32).reshape(group * cap, width)
            flat[:, chunk * width : (chunk + 1) * width] = part.astype(flat.dtype)
        hidden_of(flat, gate_w, up_w, hidden)

        def one(chunk):
            value = jnp.dot(
                hidden[...],
                down_w[:, columns_of(chunk, width)],
                preferred_element_type=jnp.float32,
            )
            outs[slot, chunk] = value.reshape(group, cap, width).astype(outs.dtype)
            landed[slot, chunk, place] = outs[slot, chunk, place]
            if send:
                give_back(slot, chunk)

        over(0, chunks, one)

    contract = (((0,), (0,)), ((), ()))

    def combine(slot, chunk):
        drain(others(landed, slot, chunk), back_recv.at[slot, chunk])
        block = landed[slot, chunk].astype(jnp.float32).reshape(group * cap, width)
        block = block.astype(jnp.bfloat16)
        value = lax.dot_general(high[slot], block, contract, preferred_element_type=jnp.float32)
        return value + lax.dot_general(
            low[slot], block, contract, preferred_element_type=jnp.float32
        )

    def pass_sum(slot, block, chunk, up):
        target = block if up else jnp.where(z - 1 == block, planes, block)
        return pltpu.make_async_remote_copy(
            src_ref=partial.at[slot, chunk],
            dst_ref=sums.at[target, chunk],
            send_sem=sum_send.at[slot, chunk],
            recv_sem=sum_recv.at[target, chunk],
            device_id=column(z + 2 * up - 1),
            device_id_type=MESH,
        )

    def reduce_one(slot, block, chunk):
        value = combine(slot, chunk)

        @pl.when(is_end)
        def _():
            partial[slot, chunk] = value.astype(partial.dtype)

        @pl.when(jnp.logical_not(is_end))
        def _():
            drain(sums.at[block, chunk], sum_recv.at[block, chunk])
            partial[slot, chunk] = (
                value + sums[block, chunk].astype(jnp.float32)
            ).astype(partial.dtype)

        @pl.when(block > z)
        def _():
            pass_sum(slot, block, chunk, 1).start()

        @pl.when(block < z)
        def _():
            pass_sum(slot, block, chunk, 0).start()

    def reduce_all(slot):
        over(0, chunks, lambda chunk: reduce_one(slot, block_of(slot), chunk))

    for chunk in range(chunks):
        tokens[z, chunk] = normed_ref[:, chunk * width : (chunk + 1) * width]
    for d in range(1, planes):
        side(d).start()
    over(0, chunks, lambda chunk: pushes(z, True, lambda up: push(z, chunk, up).start()))
    for load in loads:
        load.start()
    tables(0, side_ref[...])
    over(0, chunks, lambda chunk: pick_rows(0, z, chunk))

    for load in loads[:3]:
        load.wait()
    shared = hidden.at[pl.ds(0, tok)]
    hidden_of(normed_ref, sgate_w, sup_w, shared)

    def shared_down(chunk):
        value = jnp.dot(
            shared[...], sdown_w[:, columns_of(chunk, width)], preferred_element_type=jnp.float32
        )
        total[chunk] = value.astype(jnp.bfloat16).astype(jnp.float32)

    over(0, chunks, shared_down)
    for slot in range(1, planes):
        block = block_of(slot)
        drain(sides.at[block], side_recv.at[block])
        tables(slot, sides[block])
    collect(1)
    for load in loads[3:]:
        load.wait()
    expert(0, False)
    collect(2)
    expert(1, True)
    collect(3)
    expert(2, True)

    @pl.when(is_end)
    def _():
        reduce_all(1)

    expert(3, True)
    over(0, chunks, lambda chunk: give_back(0, chunk))

    @pl.when(is_end)
    def _():
        reduce_all(2)
        reduce_all(3)

    @pl.when(jnp.logical_not(is_end))
    def _():
        reduce_all(1)

        def one(chunk):
            reduce_one(3, block_of(3), chunk)
            reduce_one(2, block_of(2), chunk)

        over(0, chunks, one)

    def settle(chunk):
        total[chunk] += combine(0, chunk)

        @pl.when(has_down)
        def _():
            drain(sums.at[z, chunk], sum_recv.at[z, chunk])
            total[chunk] += sums[z, chunk].astype(jnp.float32)

        @pl.when(has_up)
        def _():
            drain(sums.at[planes, chunk], sum_recv.at[planes, chunk])
            total[chunk] += sums[planes, chunk].astype(jnp.float32)

    over(0, chunks, settle)
    square = jnp.zeros((tok, 1), jnp.float32)
    for chunk in range(chunks):
        value = total[chunk]
        square += jnp.sum(value * value, axis=-1, keepdims=True)
    scale = lax.rsqrt(square / (chunks * width) + epsilon)
    for chunk in range(chunks):
        some = slice(chunk * width, (chunk + 1) * width)
        o_ref[:, some] = (
            updated_ref[:, some].astype(jnp.float32) + total[chunk] * scale * gain_ref[:, some]
        ).astype(o_ref.dtype)

    for d in range(1, planes):
        side(d).wait_send()

    def sent(chunk):
        for slot in range(planes):
            block = block_of(slot)
            pushes(block, slot == 0, lambda up: push(block, chunk, up).wait_send())
            drain(others(rows, slot, chunk), out_send.at[slot, chunk])
            drain(others(outs, slot, chunk), back_send.at[slot, chunk])
            if slot:
                drain(partial.at[slot, chunk], sum_send.at[slot, chunk])

    over(0, chunks, sent)


def run_experts(planes, inner, dp_size, cap, chunks, normed, updated, side, gain, weights):
    group = inner * dp_size
    tok, model = normed.shape
    ff = weights[0].shape[1]
    width = model // chunks
    kind = normed.dtype
    blocks = pltpu.VMEM((planes, chunks, group, cap, width), kind)
    columns = pltpu.VMEM((planes, chunks, tok, width), kind)
    table = pltpu.VMEM((planes, group * cap, tok), kind)
    wide, tall = pltpu.VMEM((model, ff), kind), pltpu.VMEM((ff, model), kind)
    dma = pltpu.SemaphoreType.DMA
    return pl.pallas_call(
        functools.partial(
            experts_kernel, planes, inner, dp_size, chunks, side.shape[0] // 2
        ),
        out_shape=jax.ShapeDtypeStruct((tok, model), kind),
        in_specs=[VMEM] * 4 + [pl.BlockSpec(memory_space=pl.ANY)] * 6,
        out_specs=VMEM,
        scratch_shapes=[
            wide,
            wide,
            tall,
            wide,
            wide,
            tall,
            pltpu.VMEM((planes,) + side.shape, side.dtype),
            columns,
            pltpu.VMEM((group * cap, tok), jnp.float32),
            pltpu.VMEM((group * cap, tok), jnp.float32),
            table,
            table,
            table,
            blocks,
            blocks,
            pltpu.VMEM((group * cap, model), kind),
            pltpu.VMEM((max(group * cap, tok), ff), kind),
            blocks,
            blocks,
            columns,
            pltpu.VMEM((planes + 1, chunks, tok, width), kind),
            pltpu.VMEM((chunks, tok, width), jnp.float32),
            dma((6,)),
            dma((planes,)),
            dma((planes,)),
            dma((2, planes, chunks)),
            dma((planes, chunks)),
            dma((planes, chunks)),
            dma((planes, chunks)),
            dma((planes, chunks)),
            dma((planes, chunks)),
            dma((planes, chunks)),
            dma((planes + 1, chunks)),
        ],
        compiler_params=pltpu.CompilerParams(
            collective_id=2, has_side_effects=True, vmem_limit_bytes=56 * 2**20
        ),
    )(normed, updated, side, gain, *weights)


def local(
    queries,
    key_vectors,
    value_vectors,
    head_lambda,
    head_gain,
    residual,
    out_weight,
    mix_gain,
    pre_gain,
    post_gain,
    routes,
    route_weights,
    expert_gate,
    expert_up,
    expert_down,
    shared_gate,
    shared_up,
    shared_down,
):
    n, dp_size = lax.axis_size("sp"), lax.axis_size("dp")
    planes = 4
    inner = n // planes
    tok = queries.shape[1]
    top_count = routes.shape[2]
    cap = 3 * tok * top_count // (2 * n * dp_size)
    cap = (cap + 7) // 8 * 8
    model = residual.shape[2]
    chunks = 4

    q, k, v = to_heads(
        n,
        queries.reshape(tok, -1),
        key_vectors.reshape(tok, -1),
        value_vectors.reshape(tok, -1),
    )
    width = q.shape[2]
    attended = attend(
        q.reshape(-1, width), k.reshape(-1, width), v.reshape(-1, width), head_lambda, head_gain
    )
    flat_heads = to_tokens(n, attended.reshape(n, tok, width))

    mixed_rows = jnp.dot(flat_heads, out_weight, preferred_element_type=jnp.float32)
    updated = (residual[0].astype(jnp.float32) + rms_scale(mixed_rows, mix_gain)).astype(
        jnp.bfloat16
    )
    normed = rms_scale(updated.astype(jnp.float32), pre_gain).astype(jnp.bfloat16)
    side = jnp.concatenate([routes[0].T.astype(jnp.float32), route_weights[0].T], axis=0)
    output = run_experts(
        planes,
        inner,
        dp_size,
        cap,
        chunks,
        normed,
        updated,
        side,
        post_gain.reshape(1, -1),
        (expert_gate[0], expert_up[0], expert_down[0], shared_gate, shared_up, shared_down),
    )
    return output.reshape(1, tok, model)


def solution(mesh):
    in_specs = (
        P("dp", "sp", None, None),
        P("dp", "sp", None, None),
        P("dp", "sp", None, None),
        P("sp"),
        P(),
        P("dp", "sp", None),
        P(),
        P(),
        P(),
        P(),
        P("dp", "sp", None),
        P("dp", "sp", None),
        P(("sp", "dp"), None, None),
        P(("sp", "dp"), None, None),
        P(("sp", "dp"), None, None),
        P(),
        P(),
        P(),
    )
    out_specs = P("dp", "sp", None)
    return jax.shard_map(local, mesh=mesh, in_specs=in_specs, out_specs=out_specs, check_vma=False)
```

```python
import functools

import jax
import jax.numpy as jnp
from jax import lax
from jax.experimental import pallas as pl
from jax.experimental.pallas import tpu as pltpu
from jax.sharding import PartitionSpec as P

epsilon = 1e-06
MESH = pl.DeviceIdType.MESH
VMEM = pl.BlockSpec(memory_space=pltpu.VMEM)


def rms_scale(values_in, gain):
    return (
        values_in
        * lax.rsqrt(jnp.mean(values_in * values_in, axis=-1, keepdims=True) + epsilon)
        * gain
    )


def columns_of(index, width):
    return pl.ds(pl.multiple_of(index * width, width), width)


def line_barrier(n, me):
    barrier = pltpu.get_barrier_semaphore()

    def greet(off, carry):
        pl.semaphore_signal(
            barrier, inc=1, device_id={"sp": lax.rem(me + off, n)}, device_id_type=MESH
        )
        return carry

    lax.fori_loop(1, n, greet, 0)
    pl.semaphore_wait(barrier, n - 1)


def drain(ref, sem):
    pltpu.make_async_copy(ref, ref, sem).wait()


def attend_head(block, which_head, qkv, lam_ref, gain_ref, out):
    _, _, length, size = qkv.shape
    half = size // 2
    lane = lax.broadcasted_iota(jnp.int32, (block, size), 1)
    row = lax.broadcasted_iota(jnp.int32, (block, block), 0)
    col = lax.broadcasted_iota(jnp.int32, (block, block), 1)
    causal = col <= row
    contract = (((1,), (1,)), ((), ()))
    q_ref, k_ref, v_ref = (qkv.at[which, which_head] for which in range(3))
    for step in range(length // block):
        rows = slice(step * block, (step + 1) * block)
        past = step * block
        query = q_ref[rows, :]
        near, far = [], []
        for which in range(2):
            keep = (lane < half) if which == 0 else (lane >= half)
            part = jnp.where(keep, query, jnp.zeros_like(query))
            s_near = lax.dot_general(
                part, k_ref[rows, :], contract, preferred_element_type=jnp.float32
            ) * (half**-0.5)
            s_near = jnp.where(causal, s_near, -jnp.inf)
            top = jnp.max(s_near, axis=-1, keepdims=True)
            if past:
                s_far = lax.dot_general(
                    part, k_ref[:past, :], contract, preferred_element_type=jnp.float32
                ) * (half**-0.5)
                top = jnp.maximum(top, jnp.max(s_far, axis=-1, keepdims=True))
            e_near = jnp.exp(s_near - top)
            total = jnp.sum(e_near, axis=-1, keepdims=True)
            if past:
                e_far = jnp.exp(s_far - top)
                total = total + jnp.sum(e_far, axis=-1, keepdims=True)
            scale = 1.0 / total
            if which == 1:
                scale = scale * lam_ref[which_head]
            near.append(e_near * scale)
            if past:
                far.append(e_far * scale)
        mixture = (near[0] - near[1]).astype(jnp.bfloat16)
        result = jnp.dot(mixture, v_ref[rows, :], preferred_element_type=jnp.float32)
        if past:
            mixture = (far[0] - far[1]).astype(jnp.bfloat16)
            result += jnp.dot(mixture, v_ref[:past, :], preferred_element_type=jnp.float32)
        out[which_head, rows, :] = rms_scale(result, gain_ref[...]).astype(out.dtype)


def attention_kernel(
    n,
    q_ref,
    k_ref,
    v_ref,
    lam_ref,
    head_gain_ref,
    residual_ref,
    mix_gain_ref,
    pre_gain_ref,
    weight_hbm,
    updated_ref,
    normed_ref,
    weight,
    qkv,
    out,
    heads_in,
    mixed,
    load_sem,
    send_sem,
    recv_sem,
    back_send,
    back_recv,
):
    me = lax.axis_index("sp")
    _, heads, length, size = qkv.shape
    tok = length // n
    model = updated_ref.shape[1]
    way = 1 - 2 * (me // (n // 2))
    line_barrier(n, me)

    def loop(first, stop, action):
        lax.fori_loop(first, stop, lambda i, carry: (action(i), carry)[1], 0)

    def spot(index):
        return pl.ds(pl.multiple_of(index * tok, tok), tok)

    def to_head(head, which, off):
        dst = lax.rem(me + way * off + n, n)
        return pltpu.make_async_remote_copy(
            src_ref=(q_ref, k_ref, v_ref)[which].at[:, columns_of(dst * heads + head, size)],
            dst_ref=qkv.at[which, head, spot(me)],
            send_sem=send_sem.at[head],
            recv_sem=recv_sem.at[head],
            device_id={"sp": dst},
            device_id_type=MESH,
        )

    def to_token(head, off):
        dst = lax.rem(me + way * off + n, n)
        return pltpu.make_async_remote_copy(
            src_ref=out.at[head, spot(dst)],
            dst_ref=heads_in.at[head, :, columns_of(me, size)],
            send_sem=back_send.at[head],
            recv_sem=back_recv.at[head],
            device_id={"sp": dst},
            device_id_type=MESH,
        )

    def start_head(head):
        def one(off):
            for which in range(3):
                to_head(head, which, off).start()

        loop(1, n, one)

    for head in range(heads):
        start_head(head)

    def load(head, index):
        return pltpu.make_async_copy(
            weight_hbm.at[pl.ds(pl.multiple_of((index * heads + head) * size, size), size)],
            weight.at[head, pl.ds(pl.multiple_of(index * size, size), size)],
            load_sem.at[head],
        )

    for head in range(heads):
        loop(0, n, lambda index: load(head, index).start())
        for which, source in enumerate((q_ref, k_ref, v_ref)):
            qkv[which, head, spot(me), :] = source[:, columns_of(me * heads + head, size)]

    rest = pl.ds(0, (n - 1) * tok)

    def arrived(head):
        drain(qkv.at[:, head, rest], recv_sem.at[head])

    for head in range(heads):
        arrived(head)
        attend_head(min(256, length), head, qkv, lam_ref, head_gain_ref, out)
        loop(1, n, lambda off: to_token(head, off).start())
        heads_in[head, :, columns_of(me, size)] = out[head, spot(me), :]

    tile = min(512, model)
    for head in range(heads):
        drain(weight.at[head], load_sem.at[head])
        drain(out.at[head, rest], back_recv.at[head])

        def project(index):
            some = columns_of(index, tile)
            value = jnp.dot(
                heads_in[head], weight[head, :, some], preferred_element_type=jnp.float32
            )
            if head:
                mixed[:, some] += value
            else:
                mixed[:, some] = value

        loop(0, model // tile, project)

    value = residual_ref[...].astype(jnp.float32) + rms_scale(mixed[...], mix_gain_ref[...])
    updated_ref[...] = value.astype(updated_ref.dtype)
    normed_ref[...] = rms_scale(
        updated_ref[...].astype(jnp.float32), pre_gain_ref[...]
    ).astype(normed_ref.dtype)
    for head in range(heads):
        drain(qkv.at[:, head, rest], send_sem.at[head])
        drain(out.at[head, rest], back_send.at[head])


def run_attention(n, q, k, v, head_lambda, head_gain, residual, mix_gain, pre_gain, weight):
    tok, model = q.shape
    size = head_gain.shape[0]
    heads = model // n // size
    kind = q.dtype
    dma = pltpu.SemaphoreType.DMA
    shape = jax.ShapeDtypeStruct((tok, model), kind)
    return pl.pallas_call(
        functools.partial(attention_kernel, n),
        out_shape=[shape, shape],
        in_specs=[VMEM] * 3
        + [pl.BlockSpec(memory_space=pltpu.SMEM)]
        + [VMEM] * 4
        + [pl.BlockSpec(memory_space=pl.ANY)],
        out_specs=[VMEM] * 2,
        scratch_shapes=[
            pltpu.VMEM((heads, n * size, model), kind),
            pltpu.VMEM((3, heads, n * tok, size), kind),
            pltpu.VMEM((heads, n * tok, size), kind),
            pltpu.VMEM((heads, tok, n * size), kind),
            pltpu.VMEM((tok, model), jnp.float32),
            dma((heads,)),
            dma((heads,)),
            dma((heads,)),
            dma((heads,)),
            dma((heads,)),
        ],
        compiler_params=pltpu.CompilerParams(
            collective_id=0, has_side_effects=True, vmem_limit_bytes=56 * 2**20
        ),
    )(
        q,
        k,
        v,
        head_lambda,
        head_gain.reshape(1, -1),
        residual,
        mix_gain.reshape(1, -1),
        pre_gain.reshape(1, -1),
        weight,
    )


def experts_kernel(
    planes,
    inner,
    dp_size,
    chunks,
    top,
    normed_ref,
    updated_ref,
    side_ref,
    gain_ref,
    gate_hbm,
    up_hbm,
    down_hbm,
    sgate_hbm,
    sup_hbm,
    sdown_hbm,
    o_ref,
    gate_w,
    up_w,
    down_w,
    sgate_w,
    sup_w,
    sdown_w,
    sides,
    tokens,
    slots_a,
    slots_b,
    pick,
    high,
    low,
    rows,
    inbox,
    flat,
    hidden,
    outs,
    landed,
    partial,
    sums,
    total,
    load_sem,
    side_send,
    side_recv,
    z_send,
    z_recv,
    out_send,
    out_recv,
    back_send,
    back_recv,
    sum_send,
    sum_recv,
):
    group = inner * dp_size
    _, _, _, cap, width = rows.shape
    tok = normed_ref.shape[0]
    cores = 2 if dp_size % 2 == 0 else 1
    chips = dp_size // cores
    sp, dp = lax.axis_index("sp"), lax.axis_index("dp")
    z, y = sp // inner, lax.rem(sp, inner)
    place = y * dp_size + dp
    last = planes - 1
    has_up, has_down = z < last, z > 0
    is_end = lax.rem(z, last) == 0

    def peer(k):
        core = lax.rem(lax.rem(dp, cores) + lax.rem(k, cores), cores)
        chip = lax.rem(dp // cores + lax.rem(k // cores, chips), chips)
        row = lax.rem(y + k // dp_size, inner)
        there = chip * cores + core
        return row * dp_size + there, {"sp": z * inner + row, "dp": there}

    def column(plane):
        return {"sp": plane * inner + y, "dp": dp}

    def over(first, stop, action):
        lax.fori_loop(first, stop, lambda i, carry: (action(i), carry)[1], 0)

    barrier = pltpu.get_barrier_semaphore()
    over(
        1,
        group,
        lambda k: pl.semaphore_signal(
            barrier, inc=1, device_id=peer(k)[1], device_id_type=MESH
        ),
    )
    for d in range(1, planes):
        pl.semaphore_signal(
            barrier, inc=1, device_id=column(lax.rem(z + d, planes)), device_id_type=MESH
        )
    pl.semaphore_wait(barrier, group - 1 + planes - 1)

    loads = [
        pltpu.make_async_copy(source, target, load_sem.at[index])
        for index, (source, target) in enumerate(
            (
                (sgate_hbm, sgate_w),
                (sup_hbm, sup_w),
                (sdown_hbm, sdown_w),
                (gate_hbm, gate_w),
                (up_hbm, up_w),
                (down_hbm, down_w),
            )
        )
    ]

    def side(d):
        return pltpu.make_async_remote_copy(
            src_ref=side_ref,
            dst_ref=sides.at[z],
            send_sem=side_send.at[d],
            recv_sem=side_recv.at[z],
            device_id=column(lax.rem(z + d, planes)),
            device_id_type=MESH,
        )

    def push(block, chunk, up):
        return pltpu.make_async_remote_copy(
            src_ref=tokens.at[block, chunk],
            dst_ref=tokens.at[block, chunk],
            send_sem=z_send.at[up, block, chunk],
            recv_sem=z_recv.at[block, chunk],
            device_id=column(z + 2 * up - 1),
            device_id_type=MESH,
        )

    def pushes(block, own, action):
        @pl.when(jnp.logical_and(has_up, True if own else block < z))
        def _():
            action(1)

        @pl.when(jnp.logical_and(has_down, True if own else block > z))
        def _():
            action(0)

    def block_of(slot):
        if slot == 0:
            return z
        if slot == 1:
            return 1 + lax.rem(z, 2)
        if slot == 2:
            return lax.rem(2 + 3 * z, 5)
        return 3 * (1 - z // 2)

    def deal(slot, chunk):
        def one(k):
            there, device = peer(k)
            pltpu.make_async_remote_copy(
                src_ref=rows.at[slot, chunk, there],
                dst_ref=inbox.at[slot, chunk, place],
                send_sem=out_send.at[slot, chunk],
                recv_sem=out_recv.at[slot, chunk],
                device_id=device,
                device_id_type=MESH,
            ).start()

        over(1, group, one)

    def give_back(slot, chunk):
        def one(k):
            there, device = peer(k)
            pltpu.make_async_remote_copy(
                src_ref=outs.at[slot, chunk, there],
                dst_ref=landed.at[slot, chunk, place],
                send_sem=back_send.at[slot, chunk],
                recv_sem=back_recv.at[slot, chunk],
                device_id=device,
                device_id_type=MESH,
            ).start()

        over(1, group, one)

    def others(ref, slot, chunk):
        return ref.at[slot, chunk, pl.ds(0, group - 1)]

    def tables(slot, source):
        ids = (z * group).astype(jnp.float32) + lax.broadcasted_iota(
            jnp.int32, (group, tok), 0
        ).astype(jnp.float32)
        member = jnp.zeros((group, tok), jnp.float32)
        weight = jnp.zeros((group, tok), jnp.float32)
        for j in range(top):
            named = source[j : j + 1, :] == ids
            member += jnp.where(named, 1.0, 0.0)
            weight += jnp.where(named, source[top + j : top + j + 1, :], 0.0)
        before = lax.broadcasted_iota(jnp.int32, (tok, tok), 0) < lax.broadcasted_iota(
            jnp.int32, (tok, tok), 1
        )
        earlier = jnp.dot(
            member.astype(jnp.bfloat16),
            jnp.where(before, 1.0, 0.0).astype(jnp.bfloat16),
            preferred_element_type=jnp.float32,
        )
        rank = jnp.where(member > 0, earlier, -1.0)
        seat = lax.broadcasted_iota(jnp.int32, (cap, tok), 0).astype(jnp.float32)
        for e in range(group):
            hit = rank[e : e + 1, :] == seat
            slots_a[e * cap : (e + 1) * cap, :] = jnp.where(hit, 1.0, 0.0)
            slots_b[e * cap : (e + 1) * cap, :] = jnp.where(hit, weight[e : e + 1, :], 0.0)
        pick[slot] = slots_a[...].astype(pick.dtype)
        spread = slots_b[...]
        upper = spread.astype(high.dtype)
        high[slot] = upper
        low[slot] = (spread - upper.astype(jnp.float32)).astype(low.dtype)

    def pick_rows(slot, block, chunk):
        value = jnp.dot(pick[slot], tokens[block, chunk], preferred_element_type=jnp.float32)
        rows[slot, chunk] = value.reshape(group, cap, width).astype(rows.dtype)
        inbox[slot, chunk, place] = rows[slot, chunk, place]
        deal(slot, chunk)

    def collect(slot):
        block = block_of(slot)

        def one(chunk):
            drain(tokens.at[block, chunk], z_recv.at[block, chunk])
            pushes(block, False, lambda up: push(block, chunk, up).start())
            pick_rows(slot, block, chunk)

        over(0, chunks, one)

    tile = min(256, gate_w.shape[1])
    tiles = gate_w.shape[1] // tile

    def hidden_of(source, gates, ups, target):
        def one(index, carry):
            some = columns_of(index, tile)
            gate_val = jnp.dot(source[...], gates[:, some], preferred_element_type=jnp.float32)
            up_val = jnp.dot(source[...], ups[:, some], preferred_element_type=jnp.float32)
            target[:, some] = (jax.nn.silu(gate_val) * up_val).astype(target.dtype)
            return carry

        lax.fori_loop(0, tiles, one, 0)

    def expert(slot, send):
        for chunk in range(chunks):
            drain(others(inbox, slot, chunk), out_recv.at[slot, chunk])
            part = inbox[slot, chunk].astype(jnp.float32).reshape(group * cap, width)
            flat[:, chunk * width : (chunk + 1) * width] = part.astype(flat.dtype)
        hidden_of(flat, gate_w, up_w, hidden)

        def one(chunk):
            value = jnp.dot(
                hidden[...],
                down_w[:, columns_of(chunk, width)],
                preferred_element_type=jnp.float32,
            )
            outs[slot, chunk] = value.reshape(group, cap, width).astype(outs.dtype)
            landed[slot, chunk, place] = outs[slot, chunk, place]
            if send:
                give_back(slot, chunk)

        over(0, chunks, one)

    contract = (((0,), (0,)), ((), ()))

    def combine(slot, chunk):
        drain(others(landed, slot, chunk), back_recv.at[slot, chunk])
        block = landed[slot, chunk].astype(jnp.float32).reshape(group * cap, width)
        block = block.astype(jnp.bfloat16)
        value = lax.dot_general(high[slot], block, contract, preferred_element_type=jnp.float32)
        return value + lax.dot_general(
            low[slot], block, contract, preferred_element_type=jnp.float32
        )

    def pass_sum(slot, block, chunk, up):
        target = block if up else jnp.where(z - 1 == block, planes, block)
        return pltpu.make_async_remote_copy(
            src_ref=partial.at[slot, chunk],
            dst_ref=sums.at[target, chunk],
            send_sem=sum_send.at[slot, chunk],
            recv_sem=sum_recv.at[target, chunk],
            device_id=column(z + 2 * up - 1),
            device_id_type=MESH,
        )

    def reduce_one(slot, block, chunk):
        value = combine(slot, chunk)

        @pl.when(is_end)
        def _():
            partial[slot, chunk] = value.astype(partial.dtype)

        @pl.when(jnp.logical_not(is_end))
        def _():
            drain(sums.at[block, chunk], sum_recv.at[block, chunk])
            partial[slot, chunk] = (
                value + sums[block, chunk].astype(jnp.float32)
            ).astype(partial.dtype)

        @pl.when(block > z)
        def _():
            pass_sum(slot, block, chunk, 1).start()

        @pl.when(block < z)
        def _():
            pass_sum(slot, block, chunk, 0).start()

    def reduce_all(slot):
        over(0, chunks, lambda chunk: reduce_one(slot, block_of(slot), chunk))

    for chunk in range(chunks):
        tokens[z, chunk] = normed_ref[:, chunk * width : (chunk + 1) * width]
    for d in range(1, planes):
        side(d).start()
    over(0, chunks, lambda chunk: pushes(z, True, lambda up: push(z, chunk, up).start()))
    for load in loads:
        load.start()
    tables(0, side_ref[...])
    over(0, chunks, lambda chunk: pick_rows(0, z, chunk))

    for load in loads[:3]:
        load.wait()
    shared = hidden.at[pl.ds(0, tok)]
    hidden_of(normed_ref, sgate_w, sup_w, shared)

    def shared_down(chunk):
        value = jnp.dot(
            shared[...], sdown_w[:, columns_of(chunk, width)], preferred_element_type=jnp.float32
        )
        total[chunk] = value.astype(jnp.bfloat16).astype(jnp.float32)

    over(0, chunks, shared_down)
    for slot in range(1, planes):
        block = block_of(slot)
        drain(sides.at[block], side_recv.at[block])
        tables(slot, sides[block])
    collect(1)
    for load in loads[3:]:
        load.wait()
    expert(0, False)
    collect(2)
    expert(1, True)
    collect(3)
    expert(2, True)

    @pl.when(is_end)
    def _():
        reduce_all(1)

    expert(3, True)
    over(0, chunks, lambda chunk: give_back(0, chunk))

    @pl.when(is_end)
    def _():
        reduce_all(2)
        reduce_all(3)

    @pl.when(jnp.logical_not(is_end))
    def _():
        reduce_all(1)

        def one(chunk):
            reduce_one(3, block_of(3), chunk)
            reduce_one(2, block_of(2), chunk)

        over(0, chunks, one)

    def settle(chunk):
        total[chunk] += combine(0, chunk)

        @pl.when(has_down)
        def _():
            drain(sums.at[z, chunk], sum_recv.at[z, chunk])
            total[chunk] += sums[z, chunk].astype(jnp.float32)

        @pl.when(has_up)
        def _():
            drain(sums.at[planes, chunk], sum_recv.at[planes, chunk])
            total[chunk] += sums[planes, chunk].astype(jnp.float32)

    over(0, chunks, settle)
    square = jnp.zeros((tok, 1), jnp.float32)
    for chunk in range(chunks):
        value = total[chunk]
        square += jnp.sum(value * value, axis=-1, keepdims=True)
    scale = lax.rsqrt(square / (chunks * width) + epsilon)
    for chunk in range(chunks):
        some = slice(chunk * width, (chunk + 1) * width)
        o_ref[:, some] = (
            updated_ref[:, some].astype(jnp.float32) + total[chunk] * scale * gain_ref[:, some]
        ).astype(o_ref.dtype)

    for d in range(1, planes):
        side(d).wait_send()

    def sent(chunk):
        for slot in range(planes):
            block = block_of(slot)
            pushes(block, slot == 0, lambda up: push(block, chunk, up).wait_send())
            drain(others(rows, slot, chunk), out_send.at[slot, chunk])
            drain(others(outs, slot, chunk), back_send.at[slot, chunk])
            if slot:
                drain(partial.at[slot, chunk], sum_send.at[slot, chunk])

    over(0, chunks, sent)


def run_experts(planes, inner, dp_size, cap, chunks, normed, updated, side, gain, weights):
    group = inner * dp_size
    tok, model = normed.shape
    ff = weights[0].shape[1]
    width = model // chunks
    kind = normed.dtype
    blocks = pltpu.VMEM((planes, chunks, group, cap, width), kind)
    columns = pltpu.VMEM((planes, chunks, tok, width), kind)
    table = pltpu.VMEM((planes, group * cap, tok), kind)
    wide, tall = pltpu.VMEM((model, ff), kind), pltpu.VMEM((ff, model), kind)
    dma = pltpu.SemaphoreType.DMA
    return pl.pallas_call(
        functools.partial(
            experts_kernel, planes, inner, dp_size, chunks, side.shape[0] // 2
        ),
        out_shape=jax.ShapeDtypeStruct((tok, model), kind),
        in_specs=[VMEM] * 4 + [pl.BlockSpec(memory_space=pl.ANY)] * 6,
        out_specs=VMEM,
        scratch_shapes=[
            wide,
            wide,
            tall,
            wide,
            wide,
            tall,
            pltpu.VMEM((planes,) + side.shape, side.dtype),
            columns,
            pltpu.VMEM((group * cap, tok), jnp.float32),
            pltpu.VMEM((group * cap, tok), jnp.float32),
            table,
            table,
            table,
            blocks,
            blocks,
            pltpu.VMEM((group * cap, model), kind),
            pltpu.VMEM((max(group * cap, tok), ff), kind),
            blocks,
            blocks,
            columns,
            pltpu.VMEM((planes + 1, chunks, tok, width), kind),
            pltpu.VMEM((chunks, tok, width), jnp.float32),
            dma((6,)),
            dma((planes,)),
            dma((planes,)),
            dma((2, planes, chunks)),
            dma((planes, chunks)),
            dma((planes, chunks)),
            dma((planes, chunks)),
            dma((planes, chunks)),
            dma((planes, chunks)),
            dma((planes, chunks)),
            dma((planes + 1, chunks)),
        ],
        compiler_params=pltpu.CompilerParams(
            collective_id=2, has_side_effects=True, vmem_limit_bytes=56 * 2**20
        ),
    )(normed, updated, side, gain, *weights)


def local(
    queries,
    key_vectors,
    value_vectors,
    head_lambda,
    head_gain,
    residual,
    out_weight,
    mix_gain,
    pre_gain,
    post_gain,
    routes,
    route_weights,
    expert_gate,
    expert_up,
    expert_down,
    shared_gate,
    shared_up,
    shared_down,
):
    n, dp_size = lax.axis_size("sp"), lax.axis_size("dp")
    planes = 4
    inner = n // planes
    tok = queries.shape[1]
    top_count = routes.shape[2]
    cap = 3 * tok * top_count // (2 * n * dp_size)
    cap = (cap + 7) // 8 * 8
    model = residual.shape[2]
    chunks = 4

    updated, normed = run_attention(
        n,
        queries.reshape(tok, -1),
        key_vectors.reshape(tok, -1),
        value_vectors.reshape(tok, -1),
        head_lambda,
        head_gain,
        residual[0],
        mix_gain,
        pre_gain,
        out_weight,
    )
    side = jnp.concatenate([routes[0].T.astype(jnp.float32), route_weights[0].T], axis=0)
    output = run_experts(
        planes,
        inner,
        dp_size,
        cap,
        chunks,
        normed,
        updated,
        side,
        post_gain.reshape(1, -1),
        (expert_gate[0], expert_up[0], expert_down[0], shared_gate, shared_up, shared_down),
    )
    return output.reshape(1, tok, model)


def solution(mesh):
    in_specs = (
        P("dp", "sp", None, None),
        P("dp", "sp", None, None),
        P("dp", "sp", None, None),
        P("sp"),
        P(),
        P("dp", "sp", None),
        P(),
        P(),
        P(),
        P(),
        P("dp", "sp", None),
        P("dp", "sp", None),
        P(("sp", "dp"), None, None),
        P(("sp", "dp"), None, None),
        P(("sp", "dp"), None, None),
        P(),
        P(),
        P(),
    )
    out_specs = P("dp", "sp", None)
    return jax.shard_map(local, mesh=mesh, in_specs=in_specs, out_specs=out_specs, check_vma=False)
```

```python
import functools

import jax
import jax.numpy as jnp
from jax import lax
from jax.experimental import pallas as pl
from jax.experimental.pallas import tpu as pltpu
from jax.sharding import PartitionSpec as P

epsilon = 1e-06
MESH = pl.DeviceIdType.MESH
VMEM = pl.BlockSpec(memory_space=pltpu.VMEM)


def rms_scale(values_in, gain):
    return (
        values_in
        * lax.rsqrt(jnp.mean(values_in * values_in, axis=-1, keepdims=True) + epsilon)
        * gain
    )


def columns_of(index, width):
    return pl.ds(pl.multiple_of(index * width, width), width)


def line_barrier(n, me):
    barrier = pltpu.get_barrier_semaphore()

    def greet(off, carry):
        pl.semaphore_signal(
            barrier, inc=1, device_id={"sp": lax.rem(me + off, n)}, device_id_type=MESH
        )
        return carry

    lax.fori_loop(1, n, greet, 0)
    pl.semaphore_wait(barrier, n - 1)


def drain(ref, sem):
    pltpu.make_async_copy(ref, ref, sem).wait()


def attend_head(block, which_head, qkv, lam_ref, gain_ref, out):
    _, _, length, size = qkv.shape
    half = size // 2
    lane = lax.broadcasted_iota(jnp.int32, (block, size), 1)
    row = lax.broadcasted_iota(jnp.int32, (block, block), 0)
    col = lax.broadcasted_iota(jnp.int32, (block, block), 1)
    causal = col <= row
    contract = (((1,), (1,)), ((), ()))
    q_ref, k_ref, v_ref = (qkv.at[which, which_head] for which in range(3))
    for step in range(length // block):
        rows = slice(step * block, (step + 1) * block)
        past = step * block
        query = q_ref[rows, :]
        near, far = [], []
        for which in range(2):
            keep = (lane < half) if which == 0 else (lane >= half)
            part = jnp.where(keep, query, jnp.zeros_like(query))
            s_near = lax.dot_general(
                part, k_ref[rows, :], contract, preferred_element_type=jnp.float32
            ) * (half**-0.5)
            s_near = jnp.where(causal, s_near, -jnp.inf)
            top = jnp.max(s_near, axis=-1, keepdims=True)
            if past:
                s_far = lax.dot_general(
                    part, k_ref[:past, :], contract, preferred_element_type=jnp.float32
                ) * (half**-0.5)
                top = jnp.maximum(top, jnp.max(s_far, axis=-1, keepdims=True))
            e_near = jnp.exp(s_near - top)
            total = jnp.sum(e_near, axis=-1, keepdims=True)
            if past:
                e_far = jnp.exp(s_far - top)
                total = total + jnp.sum(e_far, axis=-1, keepdims=True)
            scale = 1.0 / total
            if which == 1:
                scale = scale * lam_ref[which_head]
            near.append(e_near * scale)
            if past:
                far.append(e_far * scale)
        mixture = (near[0] - near[1]).astype(jnp.bfloat16)
        result = jnp.dot(mixture, v_ref[rows, :], preferred_element_type=jnp.float32)
        if past:
            mixture = (far[0] - far[1]).astype(jnp.bfloat16)
            result += jnp.dot(mixture, v_ref[:past, :], preferred_element_type=jnp.float32)
        out[which_head, rows, :] = rms_scale(result, gain_ref[...]).astype(out.dtype)


def attention_kernel(
    n,
    q_ref,
    k_ref,
    v_ref,
    lam_ref,
    head_gain_ref,
    residual_ref,
    mix_gain_ref,
    pre_gain_ref,
    weight_hbm,
    updated_ref,
    normed_ref,
    weight,
    qkv,
    out,
    heads_in,
    mixed,
    load_sem,
    send_sem,
    recv_sem,
    back_send,
    back_recv,
):
    me = lax.axis_index("sp")
    _, heads, length, size = qkv.shape
    tok = length // n
    model = updated_ref.shape[1]
    way = 1 - 2 * (me // (n // 2))
    line_barrier(n, me)

    def loop(first, stop, action):
        lax.fori_loop(first, stop, lambda i, carry: (action(i), carry)[1], 0)

    def spot(index):
        return pl.ds(pl.multiple_of(index * tok, tok), tok)

    def to_head(head, which, off):
        dst = lax.rem(me + way * off + n, n)
        return pltpu.make_async_remote_copy(
            src_ref=(q_ref, k_ref, v_ref)[which].at[:, columns_of(dst * heads + head, size)],
            dst_ref=qkv.at[which, head, spot(me)],
            send_sem=send_sem.at[head],
            recv_sem=recv_sem.at[head],
            device_id={"sp": dst},
            device_id_type=MESH,
        )

    def to_token(head, off):
        dst = lax.rem(me + way * off + n, n)
        return pltpu.make_async_remote_copy(
            src_ref=out.at[head, spot(dst)],
            dst_ref=heads_in.at[head, :, columns_of(me, size)],
            send_sem=back_send.at[head],
            recv_sem=back_recv.at[head],
            device_id={"sp": dst},
            device_id_type=MESH,
        )

    def start_head(head):
        def one(off):
            for which in range(3):
                to_head(head, which, off).start()

        loop(1, n, one)

    for head in range(heads):
        start_head(head)

    def load(head, index):
        return pltpu.make_async_copy(
            weight_hbm.at[pl.ds(pl.multiple_of((index * heads + head) * size, size), size)],
            weight.at[head, pl.ds(pl.multiple_of(index * size, size), size)],
            load_sem.at[head],
        )

    for head in range(heads):
        loop(0, n, lambda index: load(head, index).start())
        for which, source in enumerate((q_ref, k_ref, v_ref)):
            qkv[which, head, spot(me), :] = source[:, columns_of(me * heads + head, size)]

    rest = pl.ds(0, (n - 1) * tok)

    def arrived(head):
        drain(qkv.at[:, head, rest], recv_sem.at[head])

    for head in range(heads):
        arrived(head)
        attend_head(min(256, length), head, qkv, lam_ref, head_gain_ref, out)
        loop(1, n, lambda off: to_token(head, off).start())
        heads_in[head, :, columns_of(me, size)] = out[head, spot(me), :]

    tile = min(512, model)
    for head in range(heads):
        drain(weight.at[head], load_sem.at[head])
        drain(out.at[head, rest], back_recv.at[head])

        def project(index):
            some = columns_of(index, tile)
            value = jnp.dot(
                heads_in[head], weight[head, :, some], preferred_element_type=jnp.float32
            )
            if head:
                mixed[:, some] += value
            else:
                mixed[:, some] = value

        loop(0, model // tile, project)

    value = residual_ref[...].astype(jnp.float32) + rms_scale(mixed[...], mix_gain_ref[...])
    updated_ref[...] = value.astype(updated_ref.dtype)
    normed_ref[...] = rms_scale(
        updated_ref[...].astype(jnp.float32), pre_gain_ref[...]
    ).astype(normed_ref.dtype)
    for head in range(heads):
        drain(qkv.at[:, head, rest], send_sem.at[head])
        drain(out.at[head, rest], back_send.at[head])


def run_attention(n, q, k, v, head_lambda, head_gain, residual, mix_gain, pre_gain, weight):
    tok, model = q.shape
    size = head_gain.shape[0]
    heads = model // n // size
    kind = q.dtype
    dma = pltpu.SemaphoreType.DMA
    shape = jax.ShapeDtypeStruct((tok, model), kind)
    return pl.pallas_call(
        functools.partial(attention_kernel, n),
        out_shape=[shape, shape],
        in_specs=[VMEM] * 3
        + [pl.BlockSpec(memory_space=pltpu.SMEM)]
        + [VMEM] * 4
        + [pl.BlockSpec(memory_space=pl.ANY)],
        out_specs=[VMEM] * 2,
        scratch_shapes=[
            pltpu.VMEM((heads, n * size, model), kind),
            pltpu.VMEM((3, heads, n * tok, size), kind),
            pltpu.VMEM((heads, n * tok, size), kind),
            pltpu.VMEM((heads, tok, n * size), kind),
            pltpu.VMEM((tok, model), jnp.float32),
            dma((heads,)),
            dma((heads,)),
            dma((heads,)),
            dma((heads,)),
            dma((heads,)),
        ],
        compiler_params=pltpu.CompilerParams(
            collective_id=0, has_side_effects=True, vmem_limit_bytes=56 * 2**20
        ),
    )(
        q,
        k,
        v,
        head_lambda,
        head_gain.reshape(1, -1),
        residual,
        mix_gain.reshape(1, -1),
        pre_gain.reshape(1, -1),
        weight,
    )


def experts_kernel(
    planes,
    inner,
    dp_size,
    chunks,
    top,
    normed_ref,
    updated_ref,
    side_ref,
    gain_ref,
    gate_hbm,
    up_hbm,
    down_hbm,
    sgate_hbm,
    sup_hbm,
    sdown_hbm,
    o_ref,
    gate_w,
    up_w,
    down_w,
    sgate_w,
    sup_w,
    sdown_w,
    sides,
    tokens,
    slots_a,
    slots_b,
    pick,
    high,
    low,
    rows,
    inbox,
    flat,
    hidden,
    outs,
    landed,
    partial,
    sums,
    total,
    load_sem,
    side_send,
    side_recv,
    z_send,
    z_recv,
    out_send,
    out_recv,
    back_send,
    back_recv,
    sum_send,
    sum_recv,
):
    group = inner * dp_size
    _, _, _, cap, width = rows.shape
    tok = normed_ref.shape[0]
    cores = 2 if dp_size % 2 == 0 else 1
    chips = dp_size // cores
    sp, dp = lax.axis_index("sp"), lax.axis_index("dp")
    z, y = sp // inner, lax.rem(sp, inner)
    place = y * dp_size + dp
    last = planes - 1
    has_up, has_down = z < last, z > 0
    is_end = lax.rem(z, last) == 0

    def peer(k):
        core = lax.rem(lax.rem(dp, cores) + lax.rem(k, cores), cores)
        chip = lax.rem(dp // cores + lax.rem(k // cores, chips), chips)
        row = lax.rem(y + k // dp_size, inner)
        there = chip * cores + core
        return row * dp_size + there, {"sp": z * inner + row, "dp": there}

    def column(plane):
        return {"sp": plane * inner + y, "dp": dp}

    def over(first, stop, action):
        lax.fori_loop(first, stop, lambda i, carry: (action(i), carry)[1], 0)

    barrier = pltpu.get_barrier_semaphore()
    over(
        1,
        group,
        lambda k: pl.semaphore_signal(
            barrier, inc=1, device_id=peer(k)[1], device_id_type=MESH
        ),
    )
    for d in range(1, planes):
        pl.semaphore_signal(
            barrier, inc=1, device_id=column(lax.rem(z + d, planes)), device_id_type=MESH
        )
    pl.semaphore_wait(barrier, group - 1 + planes - 1)

    loads = [
        pltpu.make_async_copy(source, target, load_sem.at[index])
        for index, (source, target) in enumerate(
            (
                (sgate_hbm, sgate_w),
                (sup_hbm, sup_w),
                (sdown_hbm, sdown_w),
                (gate_hbm, gate_w),
                (up_hbm, up_w),
                (down_hbm, down_w),
            )
        )
    ]

    def side(d):
        return pltpu.make_async_remote_copy(
            src_ref=side_ref,
            dst_ref=sides.at[z],
            send_sem=side_send.at[d],
            recv_sem=side_recv.at[z],
            device_id=column(lax.rem(z + d, planes)),
            device_id_type=MESH,
        )

    def push(block, chunk, up):
        return pltpu.make_async_remote_copy(
            src_ref=tokens.at[block, chunk],
            dst_ref=tokens.at[block, chunk],
            send_sem=z_send.at[up, block, chunk],
            recv_sem=z_recv.at[block, chunk],
            device_id=column(z + 2 * up - 1),
            device_id_type=MESH,
        )

    def pushes(block, own, action):
        @pl.when(jnp.logical_and(has_up, True if own else block < z))
        def _():
            action(1)

        @pl.when(jnp.logical_and(has_down, True if own else block > z))
        def _():
            action(0)

    def block_of(slot):
        if slot == 0:
            return z
        if slot == 1:
            return 1 + lax.rem(z, 2)
        if slot == 2:
            return lax.rem(2 + 3 * z, 5)
        return 3 * (1 - z // 2)

    def deal(slot, chunk):
        def one(k):
            there, device = peer(k)
            pltpu.make_async_remote_copy(
                src_ref=rows.at[slot, chunk, there],
                dst_ref=inbox.at[slot, chunk, place],
                send_sem=out_send.at[slot, chunk],
                recv_sem=out_recv.at[slot, chunk],
                device_id=device,
                device_id_type=MESH,
            ).start()

        over(1, group, one)

    def give_back(slot, first, stop):
        over(first, stop, lambda chunk: give_chunk(slot, chunk))

    def give_chunk(slot, chunk):
        def one(k):
            there, device = peer(k)
            pltpu.make_async_remote_copy(
                src_ref=outs.at[slot, chunk, there],
                dst_ref=landed.at[slot, chunk, place],
                send_sem=back_send.at[slot, chunk],
                recv_sem=back_recv.at[slot, chunk],
                device_id=device,
                device_id_type=MESH,
            ).start()

        over(1, group, one)

    def others(ref, slot, chunk):
        return ref.at[slot, chunk, pl.ds(0, group - 1)]

    def tables(slot, source):
        ids = (z * group).astype(jnp.float32) + lax.broadcasted_iota(
            jnp.int32, (group, tok), 0
        ).astype(jnp.float32)
        member = jnp.zeros((group, tok), jnp.float32)
        weight = jnp.zeros((group, tok), jnp.float32)
        for j in range(top):
            named = source[j : j + 1, :] == ids
            member += jnp.where(named, 1.0, 0.0)
            weight += jnp.where(named, source[top + j : top + j + 1, :], 0.0)
        before = lax.broadcasted_iota(jnp.int32, (tok, tok), 0) < lax.broadcasted_iota(
            jnp.int32, (tok, tok), 1
        )
        earlier = jnp.dot(
            member.astype(jnp.bfloat16),
            jnp.where(before, 1.0, 0.0).astype(jnp.bfloat16),
            preferred_element_type=jnp.float32,
        )
        rank = jnp.where(member > 0, earlier, -1.0)
        seat = lax.broadcasted_iota(jnp.int32, (cap, tok), 0).astype(jnp.float32)
        for e in range(group):
            hit = rank[e : e + 1, :] == seat
            slots_a[e * cap : (e + 1) * cap, :] = jnp.where(hit, 1.0, 0.0)
            slots_b[e * cap : (e + 1) * cap, :] = jnp.where(hit, weight[e : e + 1, :], 0.0)
        pick[slot] = slots_a[...].astype(pick.dtype)
        spread = slots_b[...]
        upper = spread.astype(high.dtype)
        high[slot] = upper
        low[slot] = (spread - upper.astype(jnp.float32)).astype(low.dtype)

    def pick_rows(slot, block, chunk):
        value = jnp.dot(pick[slot], tokens[block, chunk], preferred_element_type=jnp.float32)
        rows[slot, chunk] = value.reshape(group, cap, width).astype(rows.dtype)
        inbox[slot, chunk, place] = rows[slot, chunk, place]
        deal(slot, chunk)

    def collect(slot, first, stop):
        block = block_of(slot)

        def one(chunk):
            drain(tokens.at[block, chunk], z_recv.at[block, chunk])
            pushes(block, False, lambda up: push(block, chunk, up).start())
            pick_rows(slot, block, chunk)

        over(first, stop, one)

    tile = min(256, gate_w.shape[1])
    tiles = gate_w.shape[1] // tile

    def hidden_of(source, gates, ups, target):
        def one(index, carry):
            some = columns_of(index, tile)
            gate_val = jnp.dot(source[...], gates[:, some], preferred_element_type=jnp.float32)
            up_val = jnp.dot(source[...], ups[:, some], preferred_element_type=jnp.float32)
            target[:, some] = (jax.nn.silu(gate_val) * up_val).astype(target.dtype)
            return carry

        lax.fori_loop(0, tiles, one, 0)

    def expert(slot, send):
        for chunk in range(chunks):
            drain(others(inbox, slot, chunk), out_recv.at[slot, chunk])
            part = inbox[slot, chunk].astype(jnp.float32).reshape(group * cap, width)
            flat[:, chunk * width : (chunk + 1) * width] = part.astype(flat.dtype)
        hidden_of(flat, gate_w, up_w, hidden)

        def one(chunk):
            value = jnp.dot(
                hidden[...],
                down_w[:, columns_of(chunk, width)],
                preferred_element_type=jnp.float32,
            )
            outs[slot, chunk] = value.reshape(group, cap, width).astype(outs.dtype)
            landed[slot, chunk, place] = outs[slot, chunk, place]
            if send:
                give_chunk(slot, chunk)

        over(0, chunks, one)

    contract = (((0,), (0,)), ((), ()))

    def wait_landed(slot, first, stop):
        over(
            first,
            stop,
            lambda chunk: drain(others(landed, slot, chunk), back_recv.at[slot, chunk]),
        )

    def combine(slot, chunk):
        block = landed[slot, chunk].astype(jnp.float32).reshape(group * cap, width)
        block = block.astype(jnp.bfloat16)
        value = lax.dot_general(high[slot], block, contract, preferred_element_type=jnp.float32)
        return value + lax.dot_general(
            low[slot], block, contract, preferred_element_type=jnp.float32
        )

    def pass_sum(slot, block, chunk, up):
        target = block if up else jnp.where(z - 1 == block, planes, block)
        return pltpu.make_async_remote_copy(
            src_ref=partial.at[slot, chunk],
            dst_ref=sums.at[target, chunk],
            send_sem=sum_send.at[slot, chunk],
            recv_sem=sum_recv.at[target, chunk],
            device_id=column(z + 2 * up - 1),
            device_id_type=MESH,
        )

    def reduce_one(slot, block, chunk):
        value = combine(slot, chunk)

        @pl.when(is_end)
        def _():
            partial[slot, chunk] = value.astype(partial.dtype)

        @pl.when(jnp.logical_not(is_end))
        def _():
            drain(sums.at[block, chunk], sum_recv.at[block, chunk])
            partial[slot, chunk] = (
                value + sums[block, chunk].astype(jnp.float32)
            ).astype(partial.dtype)

        @pl.when(block > z)
        def _():
            pass_sum(slot, block, chunk, 1).start()

        @pl.when(block < z)
        def _():
            pass_sum(slot, block, chunk, 0).start()

    def reduce_some(slot, first, stop):
        over(first, stop, lambda chunk: reduce_one(slot, block_of(slot), chunk))

    for chunk in range(chunks):
        tokens[z, chunk] = normed_ref[:, chunk * width : (chunk + 1) * width]
    for d in range(1, planes):
        side(d).start()
    over(0, chunks, lambda chunk: pushes(z, True, lambda up: push(z, chunk, up).start()))
    for load in loads:
        load.start()
    tables(0, side_ref[...])
    over(0, chunks, lambda chunk: pick_rows(0, z, chunk))

    for slot in range(1, planes):
        block = block_of(slot)
        drain(sides.at[block], side_recv.at[block])
        tables(slot, sides[block])
    shared = hidden.at[pl.ds(0, tok)]
    part = max(1, chunks // 2)

    def run_shared():
        hidden_of(normed_ref, sgate_w, sup_w, shared)

        def one(chunk):
            value = jnp.dot(
                shared[...],
                sdown_w[:, columns_of(chunk, width)],
                preferred_element_type=jnp.float32,
            )
            total[chunk] = value.astype(jnp.bfloat16).astype(jnp.float32)

        over(0, chunks, one)

    collect(1, 0, chunks)
    for load in loads:
        load.wait()

    @pl.when(is_end)
    def _():
        collect(2, 0, 1)
        expert(1, False)
        give_back(1, 0, part)
        collect(2, 1, chunks)
        expert(0, False)
        collect(3, 0, part)
        wait_landed(1, 0, part)
        reduce_some(1, 0, part)
        collect(3, part, chunks)
        expert(2, False)
        run_shared()
        expert(3, True)
        give_back(2, 0, chunks)
        wait_landed(3, 0, part)
        reduce_some(3, 0, part)
        wait_landed(3, part, chunks)
        reduce_some(3, part, chunks)
        give_back(1, part, chunks)
        wait_landed(2, 0, part)
        reduce_some(2, 0, part)
        wait_landed(2, part, chunks)
        reduce_some(2, part, chunks)
        give_back(0, 0, chunks)
        wait_landed(1, part, chunks)
        reduce_some(1, part, chunks)

    @pl.when(jnp.logical_not(is_end))
    def _():
        collect(2, 0, chunks)
        expert(0, False)
        collect(3, 0, part)
        expert(1, False)
        collect(3, part, chunks)
        expert(2, False)
        expert(3, True)
        give_back(2, 0, chunks)
        give_back(1, 0, chunks)
        give_back(0, 0, chunks)
        run_shared()
        wait_landed(3, 0, chunks)
        wait_landed(2, 0, chunks)

        def one(chunk):
            reduce_one(3, block_of(3), chunk)
            reduce_one(2, block_of(2), chunk)

        over(0, chunks - 1, one)
        wait_landed(1, 0, chunks)
        reduce_some(1, 0, 1)
        over(chunks - 1, chunks, one)
        reduce_some(1, 1, chunks)

    wait_landed(0, 0, chunks)

    def settle(chunk):
        total[chunk] += combine(0, chunk)

        @pl.when(has_down)
        def _():
            drain(sums.at[z, chunk], sum_recv.at[z, chunk])
            total[chunk] += sums[z, chunk].astype(jnp.float32)

        @pl.when(has_up)
        def _():
            drain(sums.at[planes, chunk], sum_recv.at[planes, chunk])
            total[chunk] += sums[planes, chunk].astype(jnp.float32)

    over(0, chunks, settle)
    square = jnp.zeros((tok, 1), jnp.float32)
    for chunk in range(chunks):
        value = total[chunk]
        square += jnp.sum(value * value, axis=-1, keepdims=True)
    scale = lax.rsqrt(square / (chunks * width) + epsilon)
    for chunk in range(chunks):
        some = slice(chunk * width, (chunk + 1) * width)
        o_ref[:, some] = (
            updated_ref[:, some].astype(jnp.float32) + total[chunk] * scale * gain_ref[:, some]
        ).astype(o_ref.dtype)

    for d in range(1, planes):
        side(d).wait_send()

    def sent(chunk):
        for slot in range(planes):
            block = block_of(slot)
            pushes(block, slot == 0, lambda up: push(block, chunk, up).wait_send())
            drain(others(rows, slot, chunk), out_send.at[slot, chunk])
            drain(others(outs, slot, chunk), back_send.at[slot, chunk])
            if slot:
                drain(partial.at[slot, chunk], sum_send.at[slot, chunk])

    over(0, chunks, sent)


def run_experts(planes, inner, dp_size, cap, chunks, normed, updated, side, gain, weights):
    group = inner * dp_size
    tok, model = normed.shape
    ff = weights[0].shape[1]
    width = model // chunks
    kind = normed.dtype
    blocks = pltpu.VMEM((planes, chunks, group, cap, width), kind)
    columns = pltpu.VMEM((planes, chunks, tok, width), kind)
    table = pltpu.VMEM((planes, group * cap, tok), kind)
    wide, tall = pltpu.VMEM((model, ff), kind), pltpu.VMEM((ff, model), kind)
    dma = pltpu.SemaphoreType.DMA
    return pl.pallas_call(
        functools.partial(
            experts_kernel, planes, inner, dp_size, chunks, side.shape[0] // 2
        ),
        out_shape=jax.ShapeDtypeStruct((tok, model), kind),
        in_specs=[VMEM] * 4 + [pl.BlockSpec(memory_space=pl.ANY)] * 6,
        out_specs=VMEM,
        scratch_shapes=[
            wide,
            wide,
            tall,
            wide,
            wide,
            tall,
            pltpu.VMEM((planes,) + side.shape, side.dtype),
            columns,
            pltpu.VMEM((group * cap, tok), jnp.float32),
            pltpu.VMEM((group * cap, tok), jnp.float32),
            table,
            table,
            table,
            blocks,
            blocks,
            pltpu.VMEM((group * cap, model), kind),
            pltpu.VMEM((max(group * cap, tok), ff), kind),
            blocks,
            blocks,
            columns,
            pltpu.VMEM((planes + 1, chunks, tok, width), kind),
            pltpu.VMEM((chunks, tok, width), jnp.float32),
            dma((6,)),
            dma((planes,)),
            dma((planes,)),
            dma((2, planes, chunks)),
            dma((planes, chunks)),
            dma((planes, chunks)),
            dma((planes, chunks)),
            dma((planes, chunks)),
            dma((planes, chunks)),
            dma((planes, chunks)),
            dma((planes + 1, chunks)),
        ],
        compiler_params=pltpu.CompilerParams(
            collective_id=2, has_side_effects=True, vmem_limit_bytes=56 * 2**20
        ),
    )(normed, updated, side, gain, *weights)


def local(
    queries,
    key_vectors,
    value_vectors,
    head_lambda,
    head_gain,
    residual,
    out_weight,
    mix_gain,
    pre_gain,
    post_gain,
    routes,
    route_weights,
    expert_gate,
    expert_up,
    expert_down,
    shared_gate,
    shared_up,
    shared_down,
):
    n, dp_size = lax.axis_size("sp"), lax.axis_size("dp")
    planes = 4
    inner = n // planes
    tok = queries.shape[1]
    top_count = routes.shape[2]
    cap = 3 * tok * top_count // (2 * n * dp_size)
    cap = (cap + 7) // 8 * 8
    model = residual.shape[2]
    chunks = 4

    updated, normed = run_attention(
        n,
        queries.reshape(tok, -1),
        key_vectors.reshape(tok, -1),
        value_vectors.reshape(tok, -1),
        head_lambda,
        head_gain,
        residual[0],
        mix_gain,
        pre_gain,
        out_weight,
    )
    side = jnp.concatenate([routes[0].T.astype(jnp.float32), route_weights[0].T], axis=0)
    output = run_experts(
        planes,
        inner,
        dp_size,
        cap,
        chunks,
        normed,
        updated,
        side,
        post_gain.reshape(1, -1),
        (expert_gate[0], expert_up[0], expert_down[0], shared_gate, shared_up, shared_down),
    )
    return output.reshape(1, tok, model)


def solution(mesh):
    in_specs = (
        P("dp", "sp", None, None),
        P("dp", "sp", None, None),
        P("dp", "sp", None, None),
        P("sp"),
        P(),
        P("dp", "sp", None),
        P(),
        P(),
        P(),
        P(),
        P("dp", "sp", None),
        P("dp", "sp", None),
        P(("sp", "dp"), None, None),
        P(("sp", "dp"), None, None),
        P(("sp", "dp"), None, None),
        P(),
        P(),
        P(),
    )
    out_specs = P("dp", "sp", None)
    return jax.shard_map(local, mesh=mesh, in_specs=in_specs, out_specs=out_specs, check_vma=False)
```

```python
import functools

import jax
import jax.numpy as jnp
from jax import lax
from jax.experimental import pallas as pl
from jax.experimental.pallas import tpu as pltpu
from jax.sharding import PartitionSpec as P

epsilon = 1e-06
MESH = pl.DeviceIdType.MESH
VMEM = pl.BlockSpec(memory_space=pltpu.VMEM)


def rms_scale(values_in, gain):
    return (
        values_in
        * lax.rsqrt(jnp.mean(values_in * values_in, axis=-1, keepdims=True) + epsilon)
        * gain
    )


def columns_of(index, width):
    return pl.ds(pl.multiple_of(index * width, width), width)


def drain(ref, sem):
    pltpu.make_async_copy(ref, ref, sem).wait()


def attend_head(block, which_head, qkv, lam_ref, gain_ref, out):
    _, _, length, size = qkv.shape
    half = size // 2
    lane = lax.broadcasted_iota(jnp.int32, (block, size), 1)
    row = lax.broadcasted_iota(jnp.int32, (block, block), 0)
    col = lax.broadcasted_iota(jnp.int32, (block, block), 1)
    causal = col <= row
    contract = (((1,), (1,)), ((), ()))
    q_ref, k_ref, v_ref = (qkv.at[which, which_head] for which in range(3))
    for step in range(length // block):
        rows = slice(step * block, (step + 1) * block)
        past = step * block
        query = q_ref[rows, :]
        near, far = [], []
        for which in range(2):
            keep = (lane < half) if which == 0 else (lane >= half)
            part = jnp.where(keep, query, jnp.zeros_like(query))
            s_near = lax.dot_general(
                part, k_ref[rows, :], contract, preferred_element_type=jnp.float32
            ) * (half**-0.5)
            s_near = jnp.where(causal, s_near, -jnp.inf)
            top = jnp.max(s_near, axis=-1, keepdims=True)
            if past:
                s_far = lax.dot_general(
                    part, k_ref[:past, :], contract, preferred_element_type=jnp.float32
                ) * (half**-0.5)
                top = jnp.maximum(top, jnp.max(s_far, axis=-1, keepdims=True))
            e_near = jnp.exp(s_near - top)
            total = jnp.sum(e_near, axis=-1, keepdims=True)
            if past:
                e_far = jnp.exp(s_far - top)
                total = total + jnp.sum(e_far, axis=-1, keepdims=True)
            scale = 1.0 / total
            if which == 1:
                scale = scale * lam_ref[which_head]
            near.append(e_near * scale)
            if past:
                far.append(e_far * scale)
        mixture = (near[0] - near[1]).astype(jnp.bfloat16)
        result = jnp.dot(mixture, v_ref[rows, :], preferred_element_type=jnp.float32)
        if past:
            mixture = (far[0] - far[1]).astype(jnp.bfloat16)
            result += jnp.dot(mixture, v_ref[:past, :], preferred_element_type=jnp.float32)
        out[which_head, rows, :] = rms_scale(result, gain_ref[...]).astype(out.dtype)


def attention_part(
    meanwhile,
    n,
    q_ref,
    k_ref,
    v_ref,
    lam_ref,
    head_gain_ref,
    residual_ref,
    mix_gain_ref,
    pre_gain_ref,
    weight_hbm,
    updated_ref,
    normed_ref,
    weight,
    qkv,
    out,
    heads_in,
    mixed,
    load_sem,
    send_sem,
    recv_sem,
    back_send,
    back_recv,
):
    me = lax.axis_index("sp")
    _, heads, length, size = qkv.shape
    tok = length // n
    model = updated_ref.shape[1]
    way = 1 - 2 * (me // (n // 2))

    def loop(first, stop, action):
        lax.fori_loop(first, stop, lambda i, carry: (action(i), carry)[1], 0)

    def spot(index):
        return pl.ds(pl.multiple_of(index * tok, tok), tok)

    def to_head(head, which, off):
        dst = lax.rem(me + way * off + n, n)
        return pltpu.make_async_remote_copy(
            src_ref=(q_ref, k_ref, v_ref)[which].at[:, columns_of(dst * heads + head, size)],
            dst_ref=qkv.at[which, head, spot(me)],
            send_sem=send_sem.at[head],
            recv_sem=recv_sem.at[head],
            device_id={"sp": dst},
            device_id_type=MESH,
        )

    def to_token(head, off):
        dst = lax.rem(me + way * off + n, n)
        return pltpu.make_async_remote_copy(
            src_ref=out.at[head, spot(dst)],
            dst_ref=heads_in.at[head, :, columns_of(me, size)],
            send_sem=back_send.at[head],
            recv_sem=back_recv.at[head],
            device_id={"sp": dst},
            device_id_type=MESH,
        )

    def start_head(head):
        def one(off):
            for which in range(3):
                to_head(head, which, off).start()

        loop(1, n, one)

    for head in range(heads):
        start_head(head)

    def load(head, index):
        return pltpu.make_async_copy(
            weight_hbm.at[pl.ds(pl.multiple_of((index * heads + head) * size, size), size)],
            weight.at[head, pl.ds(pl.multiple_of(index * size, size), size)],
            load_sem.at[head],
        )

    for head in range(heads):
        loop(0, n, lambda index: load(head, index).start())
        for which, source in enumerate((q_ref, k_ref, v_ref)):
            qkv[which, head, spot(me), :] = source[:, columns_of(me * heads + head, size)]

    meanwhile()
    rest = pl.ds(0, (n - 1) * tok)

    def arrived(head):
        drain(qkv.at[:, head, rest], recv_sem.at[head])

    for head in range(heads):
        arrived(head)
        attend_head(min(256, length), head, qkv, lam_ref, head_gain_ref, out)
        loop(1, n, lambda off: to_token(head, off).start())
        heads_in[head, :, columns_of(me, size)] = out[head, spot(me), :]

    tile = min(512, model)
    for head in range(heads):
        drain(weight.at[head], load_sem.at[head])
        drain(out.at[head, rest], back_recv.at[head])

        def project(index):
            some = columns_of(index, tile)
            value = jnp.dot(
                heads_in[head], weight[head, :, some], preferred_element_type=jnp.float32
            )
            if head:
                mixed[:, some] += value
            else:
                mixed[:, some] = value

        loop(0, model // tile, project)

    value = residual_ref[...].astype(jnp.float32) + rms_scale(mixed[...], mix_gain_ref[...])
    updated_ref[...] = value.astype(updated_ref.dtype)
    normed_ref[...] = rms_scale(
        updated_ref[...].astype(jnp.float32), pre_gain_ref[...]
    ).astype(normed_ref.dtype)

    def finish():
        for head in range(heads):
            drain(qkv.at[:, head, rest], send_sem.at[head])
            drain(out.at[head, rest], back_send.at[head])

    return finish


def layer_kernel(
    planes,
    inner,
    dp_size,
    chunks,
    top,
    q_ref,
    k_ref,
    v_ref,
    lam_ref,
    head_gain_ref,
    residual_ref,
    mix_gain_ref,
    pre_gain_ref,
    weight_hbm,
    side_ref,
    gain_ref,
    gate_hbm,
    up_hbm,
    down_hbm,
    sgate_hbm,
    sup_hbm,
    sdown_hbm,
    o_ref,
    normed_ref,
    updated_ref,
    weight,
    qkv,
    head_out,
    heads_in,
    mixed,
    w_sem,
    q_send,
    q_recv,
    h_send,
    h_recv,
    gate_w,
    up_w,
    down_w,
    sgate_w,
    sup_w,
    sdown_w,
    sides,
    tokens,
    slots_a,
    slots_b,
    pick,
    high,
    low,
    rows,
    inbox,
    flat,
    hidden,
    outs,
    landed,
    partial,
    sums,
    total,
    load_sem,
    side_send,
    side_recv,
    z_send,
    z_recv,
    out_send,
    out_recv,
    back_send,
    back_recv,
    sum_send,
    sum_recv,
):
    group = inner * dp_size
    _, _, _, cap, width = rows.shape
    tok = normed_ref.shape[0]
    cores = 2 if dp_size % 2 == 0 else 1
    chips = dp_size // cores
    sp, dp = lax.axis_index("sp"), lax.axis_index("dp")
    z, y = sp // inner, lax.rem(sp, inner)
    place = y * dp_size + dp
    last = planes - 1
    has_up, has_down = z < last, z > 0
    is_end = lax.rem(z, last) == 0

    def peer(k):
        core = lax.rem(lax.rem(dp, cores) + lax.rem(k, cores), cores)
        chip = lax.rem(dp // cores + lax.rem(k // cores, chips), chips)
        row = lax.rem(y + k // dp_size, inner)
        there = chip * cores + core
        return row * dp_size + there, {"sp": z * inner + row, "dp": there}

    def column(plane):
        return {"sp": plane * inner + y, "dp": dp}

    def over(first, stop, action):
        lax.fori_loop(first, stop, lambda i, carry: (action(i), carry)[1], 0)

    barrier = pltpu.get_barrier_semaphore()
    over(
        1,
        group,
        lambda k: pl.semaphore_signal(
            barrier, inc=1, device_id=peer(k)[1], device_id_type=MESH
        ),
    )
    n = planes * inner
    over(
        1,
        n,
        lambda k: pl.semaphore_signal(
            barrier, inc=1, device_id={"sp": lax.rem(sp + k, n)}, device_id_type=MESH
        ),
    )
    pl.semaphore_wait(barrier, group - 1 + n - 1)

    loads = [
        pltpu.make_async_copy(source, target, load_sem.at[index])
        for index, (source, target) in enumerate(
            (
                (sgate_hbm, sgate_w),
                (sup_hbm, sup_w),
                (sdown_hbm, sdown_w),
                (gate_hbm, gate_w),
                (up_hbm, up_w),
                (down_hbm, down_w),
            )
        )
    ]

    def side(d):
        return pltpu.make_async_remote_copy(
            src_ref=side_ref,
            dst_ref=sides.at[z],
            send_sem=side_send.at[d],
            recv_sem=side_recv.at[z],
            device_id=column(lax.rem(z + d, planes)),
            device_id_type=MESH,
        )

    def push(block, chunk, up):
        return pltpu.make_async_remote_copy(
            src_ref=tokens.at[block, chunk],
            dst_ref=tokens.at[block, chunk],
            send_sem=z_send.at[up, block, chunk],
            recv_sem=z_recv.at[block, chunk],
            device_id=column(z + 2 * up - 1),
            device_id_type=MESH,
        )

    def pushes(block, own, action):
        @pl.when(jnp.logical_and(has_up, True if own else block < z))
        def _():
            action(1)

        @pl.when(jnp.logical_and(has_down, True if own else block > z))
        def _():
            action(0)

    def block_of(slot):
        if slot == 0:
            return z
        if slot == 1:
            return 1 + lax.rem(z, 2)
        if slot == 2:
            return lax.rem(2 + 3 * z, 5)
        return 3 * (1 - z // 2)

    def deal(slot, chunk):
        def one(k):
            there, device = peer(k)
            pltpu.make_async_remote_copy(
                src_ref=rows.at[slot, chunk, there],
                dst_ref=inbox.at[slot, chunk, place],
                send_sem=out_send.at[slot, chunk],
                recv_sem=out_recv.at[slot, chunk],
                device_id=device,
                device_id_type=MESH,
            ).start()

        over(1, group, one)

    def give_back(slot, first, stop):
        over(first, stop, lambda chunk: give_chunk(slot, chunk))

    def give_chunk(slot, chunk):
        def one(k):
            there, device = peer(k)
            pltpu.make_async_remote_copy(
                src_ref=outs.at[slot, chunk, there],
                dst_ref=landed.at[slot, chunk, place],
                send_sem=back_send.at[slot, chunk],
                recv_sem=back_recv.at[slot, chunk],
                device_id=device,
                device_id_type=MESH,
            ).start()

        over(1, group, one)

    def others(ref, slot, chunk):
        return ref.at[slot, chunk, pl.ds(0, group - 1)]

    def tables(slot, source):
        ids = (z * group).astype(jnp.float32) + lax.broadcasted_iota(
            jnp.int32, (group, tok), 0
        ).astype(jnp.float32)
        member = jnp.zeros((group, tok), jnp.float32)
        weight = jnp.zeros((group, tok), jnp.float32)
        for j in range(top):
            named = source[j : j + 1, :] == ids
            member += jnp.where(named, 1.0, 0.0)
            weight += jnp.where(named, source[top + j : top + j + 1, :], 0.0)
        before = lax.broadcasted_iota(jnp.int32, (tok, tok), 0) < lax.broadcasted_iota(
            jnp.int32, (tok, tok), 1
        )
        earlier = jnp.dot(
            member.astype(jnp.bfloat16),
            jnp.where(before, 1.0, 0.0).astype(jnp.bfloat16),
            preferred_element_type=jnp.float32,
        )
        rank = jnp.where(member > 0, earlier, -1.0)
        seat = lax.broadcasted_iota(jnp.int32, (cap, tok), 0).astype(jnp.float32)
        for e in range(group):
            hit = rank[e : e + 1, :] == seat
            slots_a[e * cap : (e + 1) * cap, :] = jnp.where(hit, 1.0, 0.0)
            slots_b[e * cap : (e + 1) * cap, :] = jnp.where(hit, weight[e : e + 1, :], 0.0)
        pick[slot] = slots_a[...].astype(pick.dtype)
        spread = slots_b[...]
        upper = spread.astype(high.dtype)
        high[slot] = upper
        low[slot] = (spread - upper.astype(jnp.float32)).astype(low.dtype)

    def pick_rows(slot, block, chunk):
        value = jnp.dot(pick[slot], tokens[block, chunk], preferred_element_type=jnp.float32)
        rows[slot, chunk] = value.reshape(group, cap, width).astype(rows.dtype)
        inbox[slot, chunk, place] = rows[slot, chunk, place]
        deal(slot, chunk)

    def collect(slot, first, stop):
        block = block_of(slot)

        def one(chunk):
            drain(tokens.at[block, chunk], z_recv.at[block, chunk])
            pushes(block, False, lambda up: push(block, chunk, up).start())
            pick_rows(slot, block, chunk)

        over(first, stop, one)

    tile = min(256, gate_w.shape[1])
    tiles = gate_w.shape[1] // tile

    def hidden_of(source, gates, ups, target):
        def one(index, carry):
            some = columns_of(index, tile)
            gate_val = jnp.dot(source[...], gates[:, some], preferred_element_type=jnp.float32)
            up_val = jnp.dot(source[...], ups[:, some], preferred_element_type=jnp.float32)
            target[:, some] = (jax.nn.silu(gate_val) * up_val).astype(target.dtype)
            return carry

        lax.fori_loop(0, tiles, one, 0)

    def expert(slot, send):
        for chunk in range(chunks):
            drain(others(inbox, slot, chunk), out_recv.at[slot, chunk])
            part = inbox[slot, chunk].astype(jnp.float32).reshape(group * cap, width)
            flat[:, chunk * width : (chunk + 1) * width] = part.astype(flat.dtype)
        hidden_of(flat, gate_w, up_w, hidden)

        def one(chunk):
            value = jnp.dot(
                hidden[...],
                down_w[:, columns_of(chunk, width)],
                preferred_element_type=jnp.float32,
            )
            outs[slot, chunk] = value.reshape(group, cap, width).astype(outs.dtype)
            landed[slot, chunk, place] = outs[slot, chunk, place]
            if send:
                give_chunk(slot, chunk)

        over(0, chunks, one)

    contract = (((0,), (0,)), ((), ()))

    def wait_landed(slot, first, stop):
        over(
            first,
            stop,
            lambda chunk: drain(others(landed, slot, chunk), back_recv.at[slot, chunk]),
        )

    def combine(slot, chunk):
        block = landed[slot, chunk].astype(jnp.float32).reshape(group * cap, width)
        block = block.astype(jnp.bfloat16)
        value = lax.dot_general(high[slot], block, contract, preferred_element_type=jnp.float32)
        return value + lax.dot_general(
            low[slot], block, contract, preferred_element_type=jnp.float32
        )

    def pass_sum(slot, block, chunk, up):
        target = block if up else jnp.where(z - 1 == block, planes, block)
        return pltpu.make_async_remote_copy(
            src_ref=partial.at[slot, chunk],
            dst_ref=sums.at[target, chunk],
            send_sem=sum_send.at[slot, chunk],
            recv_sem=sum_recv.at[target, chunk],
            device_id=column(z + 2 * up - 1),
            device_id_type=MESH,
        )

    def reduce_one(slot, block, chunk):
        value = combine(slot, chunk)

        @pl.when(is_end)
        def _():
            partial[slot, chunk] = value.astype(partial.dtype)

        @pl.when(jnp.logical_not(is_end))
        def _():
            drain(sums.at[block, chunk], sum_recv.at[block, chunk])
            partial[slot, chunk] = (
                value + sums[block, chunk].astype(jnp.float32)
            ).astype(partial.dtype)

        @pl.when(block > z)
        def _():
            pass_sum(slot, block, chunk, 1).start()

        @pl.when(block < z)
        def _():
            pass_sum(slot, block, chunk, 0).start()

    def reduce_some(slot, first, stop):
        over(first, stop, lambda chunk: reduce_one(slot, block_of(slot), chunk))

    def meanwhile():
        for d in range(1, planes):
            side(d).start()
        for load in loads:
            load.start()
        tables(0, side_ref[...])
        for slot in range(1, planes):
            block = block_of(slot)
            drain(sides.at[block], side_recv.at[block])
            tables(slot, sides[block])

    finish = attention_part(
        meanwhile,
        n,
        q_ref,
        k_ref,
        v_ref,
        lam_ref,
        head_gain_ref,
        residual_ref,
        mix_gain_ref,
        pre_gain_ref,
        weight_hbm,
        updated_ref,
        normed_ref,
        weight,
        qkv,
        head_out,
        heads_in,
        mixed,
        w_sem,
        q_send,
        q_recv,
        h_send,
        h_recv,
    )
    for chunk in range(chunks):
        tokens[z, chunk] = normed_ref[:, chunk * width : (chunk + 1) * width]
    over(0, chunks, lambda chunk: pushes(z, True, lambda up: push(z, chunk, up).start()))
    over(0, chunks, lambda chunk: pick_rows(0, z, chunk))
    shared = hidden.at[pl.ds(0, tok)]
    part = max(1, chunks // 2)

    def run_shared():
        hidden_of(normed_ref, sgate_w, sup_w, shared)

        def one(chunk):
            value = jnp.dot(
                shared[...],
                sdown_w[:, columns_of(chunk, width)],
                preferred_element_type=jnp.float32,
            )
            total[chunk] = value.astype(jnp.bfloat16).astype(jnp.float32)

        over(0, chunks, one)

    collect(1, 0, chunks)
    for load in loads:
        load.wait()

    @pl.when(is_end)
    def _():
        collect(2, 0, 1)
        expert(1, False)
        give_back(1, 0, part)
        collect(2, 1, chunks)
        expert(0, False)
        collect(3, 0, part)
        wait_landed(1, 0, part)
        reduce_some(1, 0, part)
        collect(3, part, chunks)
        expert(2, False)
        run_shared()
        expert(3, True)
        give_back(2, 0, chunks)
        wait_landed(3, 0, part)
        reduce_some(3, 0, part)
        wait_landed(3, part, chunks)
        reduce_some(3, part, chunks)
        give_back(1, part, chunks)
        wait_landed(2, 0, part)
        reduce_some(2, 0, part)
        wait_landed(2, part, chunks)
        reduce_some(2, part, chunks)
        give_back(0, 0, chunks)
        wait_landed(1, part, chunks)
        reduce_some(1, part, chunks)

    @pl.when(jnp.logical_not(is_end))
    def _():
        collect(2, 0, chunks)
        expert(0, False)
        collect(3, 0, part)
        expert(1, False)
        collect(3, part, chunks)
        expert(2, False)
        expert(3, True)
        give_back(2, 0, chunks)
        give_back(1, 0, chunks)
        give_back(0, 0, chunks)
        run_shared()
        wait_landed(3, 0, chunks)
        wait_landed(2, 0, chunks)

        def one(chunk):
            reduce_one(3, block_of(3), chunk)
            reduce_one(2, block_of(2), chunk)

        over(0, chunks - 1, one)
        wait_landed(1, 0, chunks)
        reduce_some(1, 0, 1)
        over(chunks - 1, chunks, one)
        reduce_some(1, 1, chunks)

    wait_landed(0, 0, chunks)

    def settle(chunk):
        total[chunk] += combine(0, chunk)

        @pl.when(has_down)
        def _():
            drain(sums.at[z, chunk], sum_recv.at[z, chunk])
            total[chunk] += sums[z, chunk].astype(jnp.float32)

        @pl.when(has_up)
        def _():
            drain(sums.at[planes, chunk], sum_recv.at[planes, chunk])
            total[chunk] += sums[planes, chunk].astype(jnp.float32)

    over(0, chunks, settle)
    square = jnp.zeros((tok, 1), jnp.float32)
    for chunk in range(chunks):
        value = total[chunk]
        square += jnp.sum(value * value, axis=-1, keepdims=True)
    scale = lax.rsqrt(square / (chunks * width) + epsilon)
    for chunk in range(chunks):
        some = slice(chunk * width, (chunk + 1) * width)
        o_ref[:, some] = (
            updated_ref[:, some].astype(jnp.float32) + total[chunk] * scale * gain_ref[:, some]
        ).astype(o_ref.dtype)

    finish()
    for d in range(1, planes):
        side(d).wait_send()

    def sent(chunk):
        for slot in range(planes):
            block = block_of(slot)
            pushes(block, slot == 0, lambda up: push(block, chunk, up).wait_send())
            drain(others(rows, slot, chunk), out_send.at[slot, chunk])
            drain(others(outs, slot, chunk), back_send.at[slot, chunk])
            if slot:
                drain(partial.at[slot, chunk], sum_send.at[slot, chunk])

    over(0, chunks, sent)


def run_layer(planes, inner, dp_size, cap, chunks, qkv, head_params, rows, out_weight, side, gain, weights):
    group = inner * dp_size
    n = planes * inner
    tok, model = qkv[0].shape
    ff = weights[0].shape[1]
    size = head_params[1].shape[1]
    heads = model // n // size
    width = model // chunks
    kind = qkv[0].dtype
    blocks = pltpu.VMEM((planes, chunks, group, cap, width), kind)
    columns = pltpu.VMEM((planes, chunks, tok, width), kind)
    table = pltpu.VMEM((planes, group * cap, tok), kind)
    wide, tall = pltpu.VMEM((model, ff), kind), pltpu.VMEM((ff, model), kind)
    flat = pltpu.VMEM((tok, model), kind)
    dma = pltpu.SemaphoreType.DMA
    anywhere = pl.BlockSpec(memory_space=pl.ANY)
    return pl.pallas_call(
        functools.partial(layer_kernel, planes, inner, dp_size, chunks, side.shape[0] // 2),
        out_shape=jax.ShapeDtypeStruct((tok, model), kind),
        in_specs=[VMEM] * 3
        + [pl.BlockSpec(memory_space=pltpu.SMEM)]
        + [VMEM] * 4
        + [anywhere]
        + [VMEM] * 2
        + [anywhere] * 6,
        out_specs=VMEM,
        scratch_shapes=[
            flat,
            flat,
            pltpu.VMEM((heads, n * size, model), kind),
            pltpu.VMEM((3, heads, n * tok, size), kind),
            pltpu.VMEM((heads, n * tok, size), kind),
            pltpu.VMEM((heads, tok, n * size), kind),
            pltpu.VMEM((tok, model), jnp.float32),
            dma((heads,)),
            dma((heads,)),
            dma((heads,)),
            dma((heads,)),
            dma((heads,)),
            wide,
            wide,
            tall,
            wide,
            wide,
            tall,
            pltpu.VMEM((planes,) + side.shape, side.dtype),
            columns,
            pltpu.VMEM((group * cap, tok), jnp.float32),
            pltpu.VMEM((group * cap, tok), jnp.float32),
            table,
            table,
            table,
            blocks,
            blocks,
            pltpu.VMEM((group * cap, model), kind),
            pltpu.VMEM((max(group * cap, tok), ff), kind),
            blocks,
            blocks,
            columns,
            pltpu.VMEM((planes + 1, chunks, tok, width), kind),
            pltpu.VMEM((chunks, tok, width), jnp.float32),
            dma((6,)),
            dma((planes,)),
            dma((planes,)),
            dma((2, planes, chunks)),
            dma((planes, chunks)),
            dma((planes, chunks)),
            dma((planes, chunks)),
            dma((planes, chunks)),
            dma((planes, chunks)),
            dma((planes, chunks)),
            dma((planes + 1, chunks)),
        ],
        compiler_params=pltpu.CompilerParams(
            collective_id=0, has_side_effects=True, vmem_limit_bytes=60 * 2**20
        ),
    )(*qkv, *head_params, *rows, out_weight, side, gain, *weights)


def local(
    queries,
    key_vectors,
    value_vectors,
    head_lambda,
    head_gain,
    residual,
    out_weight,
    mix_gain,
    pre_gain,
    post_gain,
    routes,
    route_weights,
    expert_gate,
    expert_up,
    expert_down,
    shared_gate,
    shared_up,
    shared_down,
):
    n, dp_size = lax.axis_size("sp"), lax.axis_size("dp")
    planes = 4
    inner = n // planes
    tok = queries.shape[1]
    top_count = routes.shape[2]
    cap = 3 * tok * top_count // (2 * n * dp_size)
    cap = (cap + 7) // 8 * 8
    model = residual.shape[2]
    chunks = 4

    side = jnp.concatenate([routes[0].T.astype(jnp.float32), route_weights[0].T], axis=0)
    output = run_layer(
        planes,
        inner,
        dp_size,
        cap,
        chunks,
        tuple(each.reshape(tok, -1) for each in (queries, key_vectors, value_vectors)),
        (head_lambda, head_gain.reshape(1, -1)),
        (residual[0], mix_gain.reshape(1, -1), pre_gain.reshape(1, -1)),
        out_weight,
        side,
        post_gain.reshape(1, -1),
        (expert_gate[0], expert_up[0], expert_down[0], shared_gate, shared_up, shared_down),
    )
    return output.reshape(1, tok, model)


def solution(mesh):
    in_specs = (
        P("dp", "sp", None, None),
        P("dp", "sp", None, None),
        P("dp", "sp", None, None),
        P("sp"),
        P(),
        P("dp", "sp", None),
        P(),
        P(),
        P(),
        P(),
        P("dp", "sp", None),
        P("dp", "sp", None),
        P(("sp", "dp"), None, None),
        P(("sp", "dp"), None, None),
        P(("sp", "dp"), None, None),
        P(),
        P(),
        P(),
    )
    out_specs = P("dp", "sp", None)
    return jax.shard_map(local, mesh=mesh, in_specs=in_specs, out_specs=out_specs, check_vma=False)
```

```python
import functools

import jax
import jax.numpy as jnp
from jax import lax
from jax.experimental import pallas as pl
from jax.experimental.pallas import tpu as pltpu
from jax.sharding import PartitionSpec as P

epsilon = 1e-06
MESH = pl.DeviceIdType.MESH
VMEM = pl.BlockSpec(memory_space=pltpu.VMEM)


def rms_scale(values_in, gain):
    return (
        values_in
        * lax.rsqrt(jnp.mean(values_in * values_in, axis=-1, keepdims=True) + epsilon)
        * gain
    )


def columns_of(index, width):
    return pl.ds(pl.multiple_of(index * width, width), width)


def drain(ref, sem):
    pltpu.make_async_copy(ref, ref, sem).wait()


def attend_head(block, which_head, qkv, lam_ref, gain_ref, out):
    _, _, length, size = qkv.shape
    half = size // 2
    lane = lax.broadcasted_iota(jnp.int32, (block, size), 1)
    row = lax.broadcasted_iota(jnp.int32, (block, block), 0)
    col = lax.broadcasted_iota(jnp.int32, (block, block), 1)
    causal = col <= row
    contract = (((1,), (1,)), ((), ()))
    q_ref, k_ref, v_ref = (qkv.at[which, which_head] for which in range(3))
    for step in range(length // block):
        rows = slice(step * block, (step + 1) * block)
        past = step * block
        query = q_ref[rows, :]
        near, far = [], []
        for which in range(2):
            keep = (lane < half) if which == 0 else (lane >= half)
            part = jnp.where(keep, query, jnp.zeros_like(query))
            s_near = lax.dot_general(
                part, k_ref[rows, :], contract, preferred_element_type=jnp.float32
            ) * (half**-0.5)
            s_near = jnp.where(causal, s_near, -jnp.inf)
            top = jnp.max(s_near, axis=-1, keepdims=True)
            if past:
                s_far = lax.dot_general(
                    part, k_ref[:past, :], contract, preferred_element_type=jnp.float32
                ) * (half**-0.5)
                top = jnp.maximum(top, jnp.max(s_far, axis=-1, keepdims=True))
            e_near = jnp.exp(s_near - top)
            total = jnp.sum(e_near, axis=-1, keepdims=True)
            if past:
                e_far = jnp.exp(s_far - top)
                total = total + jnp.sum(e_far, axis=-1, keepdims=True)
            scale = 1.0 / total
            if which == 1:
                scale = scale * lam_ref[which_head]
            near.append(e_near * scale)
            if past:
                far.append(e_far * scale)
        mixture = (near[0] - near[1]).astype(jnp.bfloat16)
        result = jnp.dot(mixture, v_ref[rows, :], preferred_element_type=jnp.float32)
        if past:
            mixture = (far[0] - far[1]).astype(jnp.bfloat16)
            result += jnp.dot(mixture, v_ref[:past, :], preferred_element_type=jnp.float32)
        out[which_head, rows, :] = rms_scale(result, gain_ref[...]).astype(out.dtype)


def attention_part(
    meanwhile,
    n,
    q_ref,
    k_ref,
    v_ref,
    lam_ref,
    head_gain_ref,
    residual_ref,
    mix_gain_ref,
    pre_gain_ref,
    weight_hbm,
    updated_ref,
    normed_ref,
    weight,
    qkv,
    out,
    heads_in,
    mixed,
    load_sem,
    send_sem,
    recv_sem,
    back_send,
    back_recv,
):
    me = lax.axis_index("sp")
    _, heads, length, size = qkv.shape
    tok = length // n
    model = updated_ref.shape[1]
    way = 1 - 2 * (me // (n // 2))

    def loop(first, stop, action):
        lax.fori_loop(first, stop, lambda i, carry: (action(i), carry)[1], 0)

    def spot(index):
        return pl.ds(pl.multiple_of(index * tok, tok), tok)

    def to_head(head, which, off):
        dst = lax.rem(me + way * off + n, n)
        return pltpu.make_async_remote_copy(
            src_ref=(q_ref, k_ref, v_ref)[which].at[:, columns_of(dst * heads + head, size)],
            dst_ref=qkv.at[which, head, spot(me)],
            send_sem=send_sem.at[head],
            recv_sem=recv_sem.at[head],
            device_id={"sp": dst},
            device_id_type=MESH,
        )

    def to_token(head, off):
        dst = lax.rem(me + way * off + n, n)
        return pltpu.make_async_remote_copy(
            src_ref=out.at[head, spot(dst)],
            dst_ref=heads_in.at[head, :, columns_of(me, size)],
            send_sem=back_send.at[head],
            recv_sem=back_recv.at[head],
            device_id={"sp": dst},
            device_id_type=MESH,
        )

    def start_head(head):
        def one(off):
            for which in range(3):
                to_head(head, which, off).start()

        loop(1, n, one)

    for head in range(heads):
        start_head(head)

    def load(head, index):
        return pltpu.make_async_copy(
            weight_hbm.at[pl.ds(pl.multiple_of((index * heads + head) * size, size), size)],
            weight.at[head, pl.ds(pl.multiple_of(index * size, size), size)],
            load_sem.at[head],
        )

    for head in range(heads):
        loop(0, n, lambda index: load(head, index).start())
        for which, source in enumerate((q_ref, k_ref, v_ref)):
            qkv[which, head, spot(me), :] = source[:, columns_of(me * heads + head, size)]

    meanwhile()
    rest = pl.ds(0, (n - 1) * tok)

    def arrived(head):
        drain(qkv.at[:, head, rest], recv_sem.at[head])

    for head in range(heads):
        arrived(head)
        attend_head(min(256, length), head, qkv, lam_ref, head_gain_ref, out)
        loop(1, n, lambda off: to_token(head, off).start())
        heads_in[head, :, columns_of(me, size)] = out[head, spot(me), :]

    tile = min(512, model)
    for head in range(heads):
        drain(weight.at[head], load_sem.at[head])
        drain(out.at[head, rest], back_recv.at[head])

        def project(index):
            some = columns_of(index, tile)
            value = jnp.dot(
                heads_in[head], weight[head, :, some], preferred_element_type=jnp.float32
            )
            if head:
                mixed[:, some] += value
            else:
                mixed[:, some] = value

        loop(0, model // tile, project)

    value = residual_ref[...].astype(jnp.float32) + rms_scale(mixed[...], mix_gain_ref[...])
    updated_ref[...] = value.astype(updated_ref.dtype)
    normed_ref[...] = rms_scale(
        updated_ref[...].astype(jnp.float32), pre_gain_ref[...]
    ).astype(normed_ref.dtype)

    def finish():
        for head in range(heads):
            drain(qkv.at[:, head, rest], send_sem.at[head])
            drain(out.at[head, rest], back_send.at[head])

    return finish


def layer_kernel(
    planes,
    inner,
    dp_size,
    chunks,
    top,
    q_ref,
    k_ref,
    v_ref,
    lam_ref,
    head_gain_ref,
    residual_ref,
    mix_gain_ref,
    pre_gain_ref,
    weight_hbm,
    side_ref,
    gain_ref,
    gate_hbm,
    up_hbm,
    down_hbm,
    sgate_hbm,
    sup_hbm,
    sdown_hbm,
    o_ref,
    normed_ref,
    updated_ref,
    weight,
    qkv,
    head_out,
    heads_in,
    mixed,
    w_sem,
    q_send,
    q_recv,
    h_send,
    h_recv,
    gate_w,
    up_w,
    down_w,
    sgate_w,
    sup_w,
    sdown_w,
    sides,
    tokens,
    slots_a,
    slots_b,
    pick,
    high,
    low,
    rows,
    inbox,
    flat,
    hidden,
    outs,
    landed,
    partial,
    sums,
    total,
    load_sem,
    side_send,
    side_recv,
    z_send,
    z_recv,
    out_send,
    out_recv,
    back_send,
    back_recv,
    sum_send,
    sum_recv,
):
    group = inner * dp_size
    _, _, _, cap, width = rows.shape
    tok = normed_ref.shape[0]
    cores = 2 if dp_size % 2 == 0 else 1
    chips = dp_size // cores
    sp, dp = lax.axis_index("sp"), lax.axis_index("dp")
    z, y = sp // inner, lax.rem(sp, inner)
    place = y * dp_size + dp
    last = planes - 1
    has_up, has_down = z < last, z > 0
    is_end = lax.rem(z, last) == 0

    def peer(k):
        core = lax.rem(lax.rem(dp, cores) + lax.rem(k, cores), cores)
        chip = lax.rem(dp // cores + lax.rem(k // cores, chips), chips)
        row = lax.rem(y + k // dp_size, inner)
        there = chip * cores + core
        return row * dp_size + there, {"sp": z * inner + row, "dp": there}

    def column(plane):
        return {"sp": plane * inner + y, "dp": dp}

    def over(first, stop, action):
        lax.fori_loop(first, stop, lambda i, carry: (action(i), carry)[1], 0)

    barrier = pltpu.get_barrier_semaphore()
    over(
        1,
        group,
        lambda k: pl.semaphore_signal(
            barrier, inc=1, device_id=peer(k)[1], device_id_type=MESH
        ),
    )
    n = planes * inner
    over(
        1,
        n,
        lambda k: pl.semaphore_signal(
            barrier, inc=1, device_id={"sp": lax.rem(sp + k, n)}, device_id_type=MESH
        ),
    )
    pl.semaphore_wait(barrier, group - 1 + n - 1)

    loads = [
        pltpu.make_async_copy(source, target, load_sem.at[index])
        for index, (source, target) in enumerate(
            (
                (sgate_hbm, sgate_w),
                (sup_hbm, sup_w),
                (sdown_hbm, sdown_w),
                (gate_hbm, gate_w),
                (up_hbm, up_w),
                (down_hbm, down_w),
            )
        )
    ]

    def side(d):
        return pltpu.make_async_remote_copy(
            src_ref=side_ref,
            dst_ref=sides.at[z],
            send_sem=side_send.at[d],
            recv_sem=side_recv.at[z],
            device_id=column(lax.rem(z + d, planes)),
            device_id_type=MESH,
        )

    def push(block, chunk, up):
        return pltpu.make_async_remote_copy(
            src_ref=tokens.at[block, chunk],
            dst_ref=tokens.at[block, chunk],
            send_sem=z_send.at[up, block, chunk],
            recv_sem=z_recv.at[block, chunk],
            device_id=column(z + 2 * up - 1),
            device_id_type=MESH,
        )

    def pushes(block, own, action):
        @pl.when(jnp.logical_and(has_up, True if own else block < z))
        def _():
            action(1)

        @pl.when(jnp.logical_and(has_down, True if own else block > z))
        def _():
            action(0)

    def block_of(slot):
        if slot == 0:
            return z
        if slot == 1:
            return 1 + lax.rem(z, 2)
        if slot == 2:
            return lax.rem(2 + 3 * z, 5)
        return 3 * (1 - z // 2)

    def deal(slot, chunk):
        def one(k):
            there, device = peer(k)
            pltpu.make_async_remote_copy(
                src_ref=rows.at[slot, chunk, there],
                dst_ref=inbox.at[slot, chunk, place],
                send_sem=out_send.at[slot, chunk],
                recv_sem=out_recv.at[slot, chunk],
                device_id=device,
                device_id_type=MESH,
            ).start()

        over(1, group, one)

    def give_back(slot, first, stop):
        over(first, stop, lambda chunk: give_chunk(slot, chunk))

    def give_chunk(slot, chunk):
        def one(k):
            there, device = peer(k)
            pltpu.make_async_remote_copy(
                src_ref=outs.at[slot, chunk, there],
                dst_ref=landed.at[slot, chunk, place],
                send_sem=back_send.at[slot, chunk],
                recv_sem=back_recv.at[slot, chunk],
                device_id=device,
                device_id_type=MESH,
            ).start()

        over(1, group, one)

    def others(ref, slot, chunk):
        return ref.at[slot, chunk, pl.ds(0, group - 1)]

    def tables(slot, source):
        ids = (z * group).astype(jnp.float32) + lax.broadcasted_iota(
            jnp.int32, (group, tok), 0
        ).astype(jnp.float32)
        member = jnp.zeros((group, tok), jnp.float32)
        weight = jnp.zeros((group, tok), jnp.float32)
        for j in range(top):
            named = source[j : j + 1, :] == ids
            member += jnp.where(named, 1.0, 0.0)
            weight += jnp.where(named, source[top + j : top + j + 1, :], 0.0)
        before = lax.broadcasted_iota(jnp.int32, (tok, tok), 0) < lax.broadcasted_iota(
            jnp.int32, (tok, tok), 1
        )
        earlier = jnp.dot(
            member.astype(jnp.bfloat16),
            jnp.where(before, 1.0, 0.0).astype(jnp.bfloat16),
            preferred_element_type=jnp.float32,
        )
        rank = jnp.where(member > 0, earlier, -1.0)
        seat = lax.broadcasted_iota(jnp.int32, (cap, tok), 0).astype(jnp.float32)
        for e in range(group):
            hit = rank[e : e + 1, :] == seat
            slots_a[e * cap : (e + 1) * cap, :] = jnp.where(hit, 1.0, 0.0)
            slots_b[e * cap : (e + 1) * cap, :] = jnp.where(hit, weight[e : e + 1, :], 0.0)
        pick[slot] = slots_a[...].astype(pick.dtype)
        spread = slots_b[...]
        upper = spread.astype(high.dtype)
        high[slot] = upper
        low[slot] = (spread - upper.astype(jnp.float32)).astype(low.dtype)

    def pick_rows(slot, block, chunk):
        value = jnp.dot(pick[slot], tokens[block, chunk], preferred_element_type=jnp.float32)
        rows[slot, chunk] = value.reshape(group, cap, width).astype(rows.dtype)
        inbox[slot, chunk, place] = rows[slot, chunk, place]
        deal(slot, chunk)

    def collect(slot, first, stop):
        block = block_of(slot)

        def one(chunk):
            drain(tokens.at[block, chunk], z_recv.at[block, chunk])
            pushes(block, False, lambda up: push(block, chunk, up).start())
            pick_rows(slot, block, chunk)

        over(first, stop, one)

    tile = min(256, gate_w.shape[1])
    tiles = gate_w.shape[1] // tile

    def hidden_of(source, gates, ups, target):
        def one(index, carry):
            some = columns_of(index, tile)
            gate_val = jnp.dot(source[...], gates[:, some], preferred_element_type=jnp.float32)
            up_val = jnp.dot(source[...], ups[:, some], preferred_element_type=jnp.float32)
            target[:, some] = (jax.nn.silu(gate_val) * up_val).astype(target.dtype)
            return carry

        lax.fori_loop(0, tiles, one, 0)

    def expert(slot, send):
        for chunk in range(chunks):
            drain(others(inbox, slot, chunk), out_recv.at[slot, chunk])
            part = inbox[slot, chunk].astype(jnp.float32).reshape(group * cap, width)
            flat[:, chunk * width : (chunk + 1) * width] = part.astype(flat.dtype)
        hidden_of(flat, gate_w, up_w, hidden)

        def one(chunk):
            value = jnp.dot(
                hidden[...],
                down_w[:, columns_of(chunk, width)],
                preferred_element_type=jnp.float32,
            )
            outs[slot, chunk] = value.reshape(group, cap, width).astype(outs.dtype)
            landed[slot, chunk, place] = outs[slot, chunk, place]
            if send:
                give_chunk(slot, chunk)

        over(0, chunks, one)

    contract = (((0,), (0,)), ((), ()))

    def wait_landed(slot, first, stop):
        over(
            first,
            stop,
            lambda chunk: drain(others(landed, slot, chunk), back_recv.at[slot, chunk]),
        )

    def combine(slot, chunk):
        block = landed[slot, chunk].astype(jnp.float32).reshape(group * cap, width)
        block = block.astype(jnp.bfloat16)
        value = lax.dot_general(high[slot], block, contract, preferred_element_type=jnp.float32)
        return value + lax.dot_general(
            low[slot], block, contract, preferred_element_type=jnp.float32
        )

    def pass_sum(slot, block, chunk, up):
        target = block if up else jnp.where(z - 1 == block, planes, block)
        return pltpu.make_async_remote_copy(
            src_ref=partial.at[slot, chunk],
            dst_ref=sums.at[target, chunk],
            send_sem=sum_send.at[slot, chunk],
            recv_sem=sum_recv.at[target, chunk],
            device_id=column(z + 2 * up - 1),
            device_id_type=MESH,
        )

    def reduce_one(slot, block, chunk):
        value = combine(slot, chunk)

        @pl.when(is_end)
        def _():
            partial[slot, chunk] = value.astype(partial.dtype)

        @pl.when(jnp.logical_not(is_end))
        def _():
            drain(sums.at[block, chunk], sum_recv.at[block, chunk])
            partial[slot, chunk] = (
                value + sums[block, chunk].astype(jnp.float32)
            ).astype(partial.dtype)

        @pl.when(block > z)
        def _():
            pass_sum(slot, block, chunk, 1).start()

        @pl.when(block < z)
        def _():
            pass_sum(slot, block, chunk, 0).start()

    def reduce_some(slot, first, stop):
        over(first, stop, lambda chunk: reduce_one(slot, block_of(slot), chunk))

    def meanwhile():
        for d in range(1, planes):
            side(d).start()
        for load in loads:
            load.start()
        tables(0, side_ref[...])
        for slot in range(1, planes):
            block = block_of(slot)
            drain(sides.at[block], side_recv.at[block])
            tables(slot, sides[block])

    finish = attention_part(
        meanwhile,
        n,
        q_ref,
        k_ref,
        v_ref,
        lam_ref,
        head_gain_ref,
        residual_ref,
        mix_gain_ref,
        pre_gain_ref,
        weight_hbm,
        updated_ref,
        normed_ref,
        weight,
        qkv,
        head_out,
        heads_in,
        mixed,
        w_sem,
        q_send,
        q_recv,
        h_send,
        h_recv,
    )
    for chunk in range(chunks):
        tokens[z, chunk] = normed_ref[:, chunk * width : (chunk + 1) * width]
    over(0, chunks, lambda chunk: pushes(z, True, lambda up: push(z, chunk, up).start()))
    over(0, chunks, lambda chunk: pick_rows(0, z, chunk))
    shared = hidden.at[pl.ds(0, tok)]
    part = max(1, chunks // 2)

    def run_shared():
        hidden_of(normed_ref, sgate_w, sup_w, shared)

        def one(chunk):
            value = jnp.dot(
                shared[...],
                sdown_w[:, columns_of(chunk, width)],
                preferred_element_type=jnp.float32,
            )
            total[chunk] = value.astype(jnp.bfloat16).astype(jnp.float32)

        over(0, chunks, one)

    collect(1, 0, chunks)
    for load in loads:
        load.wait()

    @pl.when(is_end)
    def _():
        collect(2, 0, 1)
        expert(1, False)
        give_back(1, 0, part)
        collect(2, 1, chunks)
        expert(0, False)
        collect(3, 0, part)
        wait_landed(1, 0, part)
        reduce_some(1, 0, part)
        collect(3, part, chunks)
        expert(2, False)
        run_shared()
        expert(3, True)
        give_back(2, 0, chunks)
        wait_landed(3, 0, part)
        reduce_some(3, 0, part)
        wait_landed(3, part, chunks)
        reduce_some(3, part, chunks)
        give_back(1, part, chunks)
        wait_landed(2, 0, part)
        reduce_some(2, 0, part)
        wait_landed(2, part, chunks)
        reduce_some(2, part, chunks)
        give_back(0, 0, chunks)
        wait_landed(1, part, chunks)
        reduce_some(1, part, chunks)

    @pl.when(jnp.logical_not(is_end))
    def _():
        collect(2, 0, chunks)
        expert(0, False)
        collect(3, 0, part)
        expert(1, False)
        collect(3, part, chunks)
        expert(2, False)
        expert(3, True)
        give_back(2, 0, chunks)
        give_back(1, 0, chunks)
        give_back(0, 0, chunks)
        run_shared()
        wait_landed(3, 0, chunks)
        wait_landed(2, 0, chunks)

        def one(chunk):
            reduce_one(3, block_of(3), chunk)
            reduce_one(2, block_of(2), chunk)

        over(0, chunks - 1, one)
        wait_landed(1, 0, chunks)
        reduce_some(1, 0, 1)
        over(chunks - 1, chunks, one)
        reduce_some(1, 1, chunks)

    wait_landed(0, 0, chunks)

    def settle(chunk):
        total[chunk] += combine(0, chunk)

        @pl.when(has_down)
        def _():
            drain(sums.at[z, chunk], sum_recv.at[z, chunk])
            total[chunk] += sums[z, chunk].astype(jnp.float32)

        @pl.when(has_up)
        def _():
            drain(sums.at[planes, chunk], sum_recv.at[planes, chunk])
            total[chunk] += sums[planes, chunk].astype(jnp.float32)

    over(0, chunks, settle)
    square = jnp.zeros((tok, 1), jnp.float32)
    for chunk in range(chunks):
        value = total[chunk]
        square += jnp.sum(value * value, axis=-1, keepdims=True)
    scale = lax.rsqrt(square / (chunks * width) + epsilon)
    for chunk in range(chunks):
        some = slice(chunk * width, (chunk + 1) * width)
        o_ref[:, some] = (
            updated_ref[:, some].astype(jnp.float32) + total[chunk] * scale * gain_ref[:, some]
        ).astype(o_ref.dtype)

    finish()
    for d in range(1, planes):
        side(d).wait_send()

    def sent(chunk):
        for slot in range(planes):
            block = block_of(slot)
            pushes(block, slot == 0, lambda up: push(block, chunk, up).wait_send())
            drain(others(rows, slot, chunk), out_send.at[slot, chunk])
            drain(others(outs, slot, chunk), back_send.at[slot, chunk])
            if slot:
                drain(partial.at[slot, chunk], sum_send.at[slot, chunk])

    over(0, chunks, sent)


def run_layer(planes, inner, dp_size, cap, chunks, qkv, head_params, rows, out_weight, side, gain, weights):
    group = inner * dp_size
    n = planes * inner
    tok, model = qkv[0].shape
    ff = weights[0].shape[1]
    size = head_params[1].shape[1]
    heads = model // n // size
    width = model // chunks
    kind = qkv[0].dtype
    blocks = pltpu.VMEM((planes, chunks, group, cap, width), kind)
    columns = pltpu.VMEM((planes, chunks, tok, width), kind)
    table = pltpu.VMEM((planes, group * cap, tok), kind)
    wide, tall = pltpu.VMEM((model, ff), kind), pltpu.VMEM((ff, model), kind)
    flat = pltpu.VMEM((tok, model), kind)
    dma = pltpu.SemaphoreType.DMA
    anywhere = pl.BlockSpec(memory_space=pl.ANY)
    return pl.pallas_call(
        functools.partial(layer_kernel, planes, inner, dp_size, chunks, side.shape[0] // 2),
        out_shape=jax.ShapeDtypeStruct((tok, model), kind),
        in_specs=[VMEM] * 3
        + [pl.BlockSpec(memory_space=pltpu.SMEM)]
        + [VMEM] * 4
        + [anywhere]
        + [VMEM] * 2
        + [anywhere] * 6,
        out_specs=VMEM,
        scratch_shapes=[
            flat,
            flat,
            pltpu.VMEM((heads, n * size, model), kind),
            pltpu.VMEM((3, heads, n * tok, size), kind),
            pltpu.VMEM((heads, n * tok, size), kind),
            pltpu.VMEM((heads, tok, n * size), kind),
            pltpu.VMEM((tok, model), jnp.float32),
            dma((heads,)),
            dma((heads,)),
            dma((heads,)),
            dma((heads,)),
            dma((heads,)),
            wide,
            wide,
            tall,
            wide,
            wide,
            tall,
            pltpu.VMEM((planes,) + side.shape, side.dtype),
            columns,
            pltpu.VMEM((group * cap, tok), jnp.float32),
            pltpu.VMEM((group * cap, tok), jnp.float32),
            table,
            table,
            table,
            blocks,
            blocks,
            pltpu.VMEM((group * cap, model), kind),
            pltpu.VMEM((max(group * cap, tok), ff), kind),
            blocks,
            blocks,
            columns,
            pltpu.VMEM((planes + 1, chunks, tok, width), kind),
            pltpu.VMEM((chunks, tok, width), jnp.float32),
            dma((6,)),
            dma((planes,)),
            dma((planes,)),
            dma((2, planes, chunks)),
            dma((planes, chunks)),
            dma((planes, chunks)),
            dma((planes, chunks)),
            dma((planes, chunks)),
            dma((planes, chunks)),
            dma((planes, chunks)),
            dma((planes + 1, chunks)),
        ],
        compiler_params=pltpu.CompilerParams(
            collective_id=0, has_side_effects=True, vmem_limit_bytes=40 * 2**20 + n * tok * 10 * 2**10
        ),
    )(*qkv, *head_params, *rows, out_weight, side, gain, *weights)


def local(
    queries,
    key_vectors,
    value_vectors,
    head_lambda,
    head_gain,
    residual,
    out_weight,
    mix_gain,
    pre_gain,
    post_gain,
    routes,
    route_weights,
    expert_gate,
    expert_up,
    expert_down,
    shared_gate,
    shared_up,
    shared_down,
):
    n, dp_size = lax.axis_size("sp"), lax.axis_size("dp")
    planes = 4
    inner = n // planes
    tok = queries.shape[1]
    top_count = routes.shape[2]
    cap = 3 * tok * top_count // (2 * n * dp_size)
    cap = (cap + 7) // 8 * 8
    model = residual.shape[2]
    chunks = 4

    side = jnp.concatenate([routes[0].T.astype(jnp.float32), route_weights[0].T], axis=0)
    output = run_layer(
        planes,
        inner,
        dp_size,
        cap,
        chunks,
        tuple(each.reshape(tok, -1) for each in (queries, key_vectors, value_vectors)),
        (head_lambda, head_gain.reshape(1, -1)),
        (residual[0], mix_gain.reshape(1, -1), pre_gain.reshape(1, -1)),
        out_weight,
        side,
        post_gain.reshape(1, -1),
        (expert_gate[0], expert_up[0], expert_down[0], shared_gate, shared_up, shared_down),
    )
    return output.reshape(1, tok, model)


def solution(mesh):
    in_specs = (
        P("dp", "sp", None, None),
        P("dp", "sp", None, None),
        P("dp", "sp", None, None),
        P("sp"),
        P(),
        P("dp", "sp", None),
        P(),
        P(),
        P(),
        P(),
        P("dp", "sp", None),
        P("dp", "sp", None),
        P(("sp", "dp"), None, None),
        P(("sp", "dp"), None, None),
        P(("sp", "dp"), None, None),
        P(),
        P(),
        P(),
    )
    out_specs = P("dp", "sp", None)
    return jax.shard_map(local, mesh=mesh, in_specs=in_specs, out_specs=out_specs, check_vma=False)
```
